128 devices in a mesh: sp: 16 (over z, y), tp: 8 (over x, core).
Axes of the slice: x: 4, y: 4, z: 4, core: 2. Of those that a mesh axis runs over, the one named last changes fastest.
Arguments:
- query_proj: bfloat16 [16384, 2048], P('sp', 'tp'), may hold values from -6 to 6
- key_proj: bfloat16 [16384, 2048], P('sp', 'tp'), may hold values from -6 to 6
- value_proj: bfloat16 [16384, 4096], P('sp', 'tp'), may hold values from -6 to 6
- gate_proj: bfloat16 [16384, 4096], P('sp', 'tp'), may hold values from -6 to 6
- log_decay: float32 [16384, 8], P('sp', 'tp'), may hold values from -0.75 to 0, as said below
- residual: bfloat16 [16384, 2048], P('sp'), may hold values from -4 to 4
- out_weight: bfloat16 [4096, 2048], P('tp'), may hold values from -0.09375 to 0.09375
- norm_gain: float32 [2, 2048], replicated, may hold values from 0.1 to 1.9
- norm_bias: float32 [2, 2048], replicated, may hold values from -1.5 to 1.5
- up_gate: bfloat16 [2048, 5632], P('sp', 'tp'), may hold values from -0.125 to 0.125
- up_value: bfloat16 [2048, 5632], P('sp', 'tp'), may hold values from -0.125 to 0.125
- conv_weight: float32 [2, 3, 5632], P(None, None, 'tp'), may hold values from -3 to 3
- conv_bias: float32 [2, 5632], P(None, 'tp'), may hold values from -1.5 to 1.5
- down_weight: bfloat16 [5632, 2048], P('tp', 'sp'), may hold values from -0.078125 to 0.078125
Outputs:
- layer_output: bfloat16 [16384, 2048], P(('sp', 'tp'))
The draws below stay inside these ranges and needn't reach their ends.
Inputs may be any that keep to these rules, and one draw needn't show every extreme that they name: `log_decay`: all entries are negative.
All inputs are finite; a program needn't handle non-finite values.
Results may differ from the reference program's by a relative error of at most 0.023.
Values may be sent and summed in bfloat16 or wider, within the bound.
A program may use at most 128 MiB of HBM per device.

```python
import math
import jax
import jax.numpy as jnp
from jax import lax

D = 2048
RETENTION_HEADS = 8
DK = 256
DV = 512
FF = 5632
BLOCK = 256
TOK_DEV = 1024
SEQUENCE_TOKENS = 16384
N_TP = 8


def draw_log_decay(key, part):
    random_keys = jax.random.split(jax.random.fold_in(key, 71), 7)
    fast_limit = 5
    quick_decay_heads = jax.random.randint(random_keys[0], (RETENTION_HEADS,), 0, 10) < fast_limit
    fast_span = jax.random.uniform(random_keys[1], (RETENTION_HEADS,), jnp.float32, 30.0, 50.0)
    slow_rate = -0.2 / SEQUENCE_TOKENS * jax.random.uniform(random_keys[2], (RETENTION_HEADS,), jnp.float32, 0.5, 1.0)
    decay_base_rate = jnp.where(quick_decay_heads, -math.log(10.0) / fast_span, slow_rate)
    device_count = SEQUENCE_TOKENS // TOK_DEV
    replica_multiplier = jnp.exp(jax.random.uniform(random_keys[3], (device_count, RETENTION_HEADS), jnp.float32, math.log(0.5), math.log(2.0)))
    replica_multiplier = jnp.repeat(replica_multiplier, TOK_DEV, axis=0)
    jitter_amount = jax.random.uniform(random_keys[4], (SEQUENCE_TOKENS, RETENTION_HEADS), jnp.float32, 0.5, 1.5)
    spike_positions = jax.random.randint(random_keys[5], (2, RETENTION_HEADS), 0, SEQUENCE_TOKENS)
    spike_lengths = jax.random.uniform(random_keys[6], (2, RETENTION_HEADS), jnp.float32, math.log(0.5), math.log(0.8))
    position_slots = jnp.arange(SEQUENCE_TOKENS)[:, None]
    spike_events = jnp.where(position_slots == spike_positions[0][None, :], spike_lengths[0][None, :], 0.0)
    spike_events = spike_events + jnp.where(position_slots == spike_positions[1][None, :], spike_lengths[1][None, :], 0.0)
    spike_events = jnp.where(quick_decay_heads[None, :], 0.0, spike_events)
    return (decay_base_rate[None, :] * replica_multiplier * jitter_amount + spike_events).astype(jnp.float32)


def shard_levels(rng, extent, cuts, least, largest):
    def one(position, parts):
        steps = jax.random.uniform(jax.random.fold_in(jax.random.fold_in(rng, 6), position), (parts,), jnp.float32, least / len(cuts), largest / len(cuts))
        return jnp.repeat(jnp.exp(steps), extent[position] // parts).reshape((-1,) + (1,) * (len(extent) - position - 1))

    loudness = one(*cuts[0])
    for cut in cuts[1:]:
        loudness = loudness * one(*cut)
    return loudness


def normal_values(own_key, dims, deviation, limit, cuts=(), held_as=jnp.bfloat16):
    values = jax.random.normal(own_key, dims, jnp.float32) * deviation
    if len(cuts) > 0:
        values = shard_levels(own_key, dims, cuts, -0.22, 0.18) * values
    return jnp.clip(values, min=-limit, max=limit).astype(held_as)


def setup_inputs(seed: int = 0) -> dict:
    splits = jax.random.split(jax.random.key(seed), 15)
    query_proj = normal_values(splits[0], (SEQUENCE_TOKENS, RETENTION_HEADS * DK), 1.0, 6.0, ((0, 16), (1, 8)))
    key_proj = normal_values(splits[1], (SEQUENCE_TOKENS, RETENTION_HEADS * DK), 1.0, 6.0, ((0, 16), (1, 8)))
    value_proj = normal_values(splits[2], (SEQUENCE_TOKENS, RETENTION_HEADS * DV), 1.0, 6.0, ((0, 16), (1, 8)))
    gate_proj = normal_values(splits[3], (SEQUENCE_TOKENS, RETENTION_HEADS * DV), 1.0, 6.0, ((0, 16), (1, 8)))
    log_decay = draw_log_decay(jax.random.fold_in(splits[14], 71), 0)
    residual = normal_values(splits[5], (SEQUENCE_TOKENS, D), 0.5, 4.0, ((0, 16),))
    out_weight = normal_values(splits[6], (RETENTION_HEADS * DV, D), (RETENTION_HEADS * DV) ** -0.5, 0.09375, ((0, 8),))
    norm_gain = jnp.clip(1.0 + 0.18 * jax.random.normal(splits[7], (2, D), jnp.float32), 0.1, 1.9)
    norm_bias = normal_values(splits[8], (2, D), 0.3, 1.5, (), jnp.float32)
    up_gate = normal_values(splits[9], (D, FF), D ** -0.5, 0.125, ((0, 16), (1, 8)))
    up_value = normal_values(splits[10], (D, FF), D ** -0.5, 0.125, ((0, 16), (1, 8)))
    conv_weight = normal_values(splits[11], (2, 3, FF), 0.577, 3.0, ((2, 8),), jnp.float32)
    conv_bias = normal_values(splits[12], (2, FF), 0.3, 1.5, ((1, 8),), jnp.float32)
    down_weight = normal_values(splits[13], (FF, D), FF ** -0.5, 0.078125, ((0, 8), (1, 16)))
    return dict(query_proj=query_proj, key_proj=key_proj, value_proj=value_proj, gate_proj=gate_proj, log_decay=log_decay, residual=residual, out_weight=out_weight, norm_gain=norm_gain, norm_bias=norm_bias, up_gate=up_gate, up_value=up_value, conv_weight=conv_weight, conv_bias=conv_bias, down_weight=down_weight)


alpha_scale = 8.0 ** 0.25
rope_base = 10000.0
tiny_stabilizer = 1e-05

def rotate(vectors, positions):
    head_width = vectors.shape[-1]
    half_width = head_width // 2
    inverse_freq = rope_base ** (-2.0 * jnp.arange(half_width, dtype=jnp.float32) / head_width)
    angles = positions[:, None] * inverse_freq[None, :]
    cosine = jnp.cos(angles)[:, None, :]
    sine_part = jnp.sin(angles)[:, None, :]
    front = vectors[..., :half_width]
    second = vectors[..., half_width:]
    return jnp.concatenate([front * cosine - second * sine_part, front * sine_part + second * cosine], axis=-1)

def layer_norm(values, gain, shift):
    average = values.mean(-1, keepdims=True)
    spread = jnp.square(values - average).mean(-1, keepdims=True)
    return (values - average) * lax.rsqrt(spread + tiny_stabilizer) * gain + shift

def rounded(values):
    return lax.optimization_barrier(values.astype(jnp.bfloat16)).astype(jnp.float32)

def block_parts(query_tile, lookup_piece, payload_piece, log_blk):
    cum_log = jnp.cumsum(log_blk, axis=0)
    cum_heads = cum_log.T
    log_gap = cum_heads[:, :, None] - cum_heads[:, None, :]
    offsets = jnp.arange(log_blk.shape[0])
    causal = (offsets[:, None] >= offsets[None, :])[None]
    weight = jnp.where(causal, jnp.exp(jnp.where(causal, log_gap, 0.0)), 0.0)
    score_matrix = jnp.einsum('jka,ska->kjs', query_tile.astype(jnp.float32), lookup_piece.astype(jnp.float32))
    segment_scaling = (score_matrix * weight).astype(jnp.bfloat16)
    within = jnp.einsum('htm,mhe->the', segment_scaling.astype(jnp.float32), payload_piece.astype(jnp.float32))
    block_total = cum_log[-1]
    to_end = jnp.exp(block_total[None, :] - cum_log)
    faded_lookup_vector = rounded(lookup_piece.astype(jnp.float32) * to_end[:, :, None])
    summand_term = jnp.einsum('ajo,ajd->jod', faded_lookup_vector, payload_piece.astype(jnp.float32), precision=lax.Precision.HIGHEST)
    scaled_query = rounded(query_tile.astype(jnp.float32) * jnp.exp(cum_log)[:, :, None])
    return (within, scaled_query, summand_term, jnp.exp(block_total))

def grouped_product(left, right, group_count):
    group_width = left.shape[1] // group_count
    left_groups = left.reshape(left.shape[0], group_count, group_width).transpose(1, 0, 2)
    right_groups = right.reshape(group_count, group_width, right.shape[1])

    def add_group(total, pieces):
        term = jnp.dot(pieces[0], pieces[1], preferred_element_type=jnp.float32).astype(jnp.bfloat16)
        return (total + term.astype(jnp.float32), None)
    blank_sum = jnp.zeros((left.shape[0], right.shape[1]), jnp.float32)
    total, _ = lax.scan(add_group, blank_sum, (left_groups, right_groups))
    return total

def causal_conv(rows, taps, shift):
    padded = jnp.pad(rows.astype(jnp.float32), ((2, 0), (0, 0)))
    length = rows.shape[0]
    result = shift[None, :] + padded[0:length] * taps[0]
    result = result + padded[1:length + 1] * taps[1]
    return result + padded[2:length + 2] * taps[2]

def reference(query_proj, key_proj, value_proj, gate_proj, log_decay, residual, out_weight, norm_gain, norm_bias, up_gate, up_value, conv_weight, conv_bias, down_weight):
    length = query_proj.shape[0]
    positions = jnp.arange(length).astype(jnp.float32)
    query_rot = rotate(query_proj.astype(jnp.float32).reshape(length, RETENTION_HEADS, DK), positions).astype(jnp.bfloat16)
    key_rot = (rotate(key_proj.astype(jnp.float32).reshape(length, RETENTION_HEADS, DK), positions) * DK ** (-0.5)).astype(jnp.bfloat16)
    block_count = length // BLOCK
    asking_segments = query_rot.reshape(block_count, BLOCK, RETENTION_HEADS, DK)
    key_blocks = key_rot.reshape(block_count, BLOCK, RETENTION_HEADS, DK)
    value_blocks = value_proj.reshape(block_count, BLOCK, RETENTION_HEADS, DV)
    log_blocks = log_decay.reshape(block_count, BLOCK, RETENTION_HEADS)

    def advance(carry_state, pieces):
        within, scaled_query, summand_term, block_decay = block_parts(*pieces)
        carried = jnp.einsum('thd,hde->the', scaled_query, rounded(carry_state), precision=lax.Precision.HIGHEST)
        return (block_decay[:, None, None] * carry_state + summand_term, within + carried)
    start_state = jnp.zeros((RETENTION_HEADS, DK, DV), jnp.float32)
    _, mixed_heads = lax.scan(advance, start_state, (asking_segments, key_blocks, value_blocks, log_blocks))
    mixed_heads = mixed_heads.reshape(length, RETENTION_HEADS, DV)
    average = mixed_heads.mean(-1, keepdims=True)
    spread = jnp.square(mixed_heads - average).mean(-1, keepdims=True)
    standardized_rows = (mixed_heads - average) * lax.rsqrt(spread + tiny_stabilizer)
    gate_heads = gate_proj.astype(jnp.float32).reshape(length, RETENTION_HEADS, DV)
    gated_rows = (jax.nn.silu(gate_heads) * standardized_rows).astype(jnp.bfloat16).reshape(length, RETENTION_HEADS * DV)
    attended = grouped_product(gated_rows, out_weight, N_TP)
    normed_rows = layer_norm(alpha_scale * residual.astype(jnp.float32) + attended, norm_gain[0], norm_bias[0]).astype(jnp.bfloat16)
    gate_up = jnp.dot(normed_rows, up_gate, preferred_element_type=jnp.float32).astype(jnp.bfloat16)
    value_up = jnp.dot(normed_rows, up_value, preferred_element_type=jnp.float32).astype(jnp.bfloat16)
    gate_conv = causal_conv(gate_up, conv_weight[0], conv_bias[0])
    value_conv = causal_conv(value_up, conv_weight[1], conv_bias[1])
    activated = (jax.nn.gelu(gate_conv) * value_conv).astype(jnp.bfloat16)
    ffn_out = grouped_product(activated, down_weight, N_TP)
    return layer_norm(alpha_scale * normed_rows.astype(jnp.float32) + ffn_out, norm_gain[1], norm_bias[1]).astype(jnp.bfloat16)
```

```python
import functools

import jax
import jax.numpy as jnp
import numpy as np
from jax import lax
from jax.experimental import pallas as pl
from jax.experimental.pallas import tpu as pltpu
from jax.sharding import Mesh
from jax.sharding import PartitionSpec as P

F32 = jnp.float32
BF16 = jnp.bfloat16
HIGH = lax.Precision.HIGHEST
MESH = pl.DeviceIdType.MESH
ALPHA = 8.0**0.25
EPS = 1e-05
NSP = 16
BLK = 256
FF = 704
FFP = 768
NT = (((1,), (1,)), ((), ()))
TN = (((0,), (0,)), ((), ()))


def position_tables():
    freq = 10000.0 ** (-2.0 * np.arange(128, dtype=np.float64) / 256.0)
    inner = np.arange(BLK, dtype=np.float64)[:, None] * freq[None]
    start = np.arange(4 * NSP, dtype=np.float64)[:, None] * BLK * freq[None]
    ti = np.stack([np.cos(inner), np.sin(inner)]).astype(np.float32)
    tb = np.concatenate(
        [np.cos(start).reshape(NSP, 4, 128), np.sin(start).reshape(NSP, 4, 128)], axis=1
    ).astype(np.float32)
    return ti, tb


def body(
    q_h, k_h, v_h, g_h, log_ref, res_h, ow_h, gain_ref, bias_ref, ug_h, uv_h, taps_ref, dw_h,
    ti_ref, tb_ref, o_ref,
    qv, kv, vv, gv, rv, owv, ust, wu, wd,
    lsc, crow, ccol, dpre, kr, sq, loc, within, gr,
    ssend, srecv, rsend, inc,
    part, d2, cb, ra, rb, rl, rr,
    xb, ub, act, halo,
    in_sem, ss_s, ss_r, rs_s, rs_r, wg_s, wg_r, d2_s, d2_r, x_s, x_r, ag_s, ag_r, h_s, h_r,
):
    z, y, x, c = (lax.axis_index(a) for a in ("z", "y", "x", "c"))
    me = z * 4 + y
    t = x * 2 + c
    xr, xl, xo = lax.rem(x + 1, 4), lax.rem(x + 3, 4), lax.rem(x + 2, 4)

    def at(axis, value):
        return {axis: value}

    SIB = at("c", 1 - c)
    XR, XL = at("x", xr), at("x", xl)

    def remote(src, dst, ssem, rsem, dev):
        return pltpu.make_async_remote_copy(
            src_ref=src, dst_ref=dst, send_sem=ssem, recv_sem=rsem, device_id=dev,
            device_id_type=MESH,
        )

    loads = [
        (ug_h.at[0:640], ust.at[0:640]),
        (uv_h.at[0:640], ust.at[640:1280]),
        (ug_h.at[640:704], ust.at[1280:1344]),
        (uv_h.at[640:704], ust.at[1344:1408]),
        (dw_h, wd.at[0:FF, pl.ds(pl.multiple_of(me * 128, 128), 128)]),
        (k_h, kv),
        (v_h, vv),
        (q_h, qv),
        (g_h, gv),
        (ow_h, owv),
        (res_h.at[pl.ds(pl.multiple_of(t * 128, 128), 128)], rv),
    ]
    loads = [pltpu.make_async_copy(s, d, in_sem.at[i]) for i, (s, d) in enumerate(loads)]
    for load in loads:
        load.start()

    barrier = pltpu.get_barrier_semaphore()

    def sp_peer(i):
        j = lax.rem(me + i, NSP)
        return j, {"z": lax.div(j, 4), "y": lax.rem(j, 4)}

    def greet(i, carry):
        _, dev = sp_peer(i)
        pl.semaphore_signal(barrier, inc=1, device_id=dev, device_id_type=MESH)
        return carry

    lax.fori_loop(1, NSP, greet, 0)
    for dev in (SIB, XR, XL):
        pl.semaphore_signal(barrier, inc=1, device_id=dev, device_id_type=MESH)

    yr, yl, yo = lax.rem(y + 1, 4), lax.rem(y + 3, 4), lax.rem(y + 2, 4)
    zr, zl, zo = lax.rem(z + 1, 4), lax.rem(z + 3, 4), lax.rem(z + 2, 4)
    YR, YL, ZR, ZL = at("y", yr), at("y", yl), at("z", zr), at("z", zl)

    def up_piece(zz, yy, lo, n):
        return wu.at[zz * 4 + yy, lo * 16 : (lo + n) * 16, :]

    def dn_piece(zz, yy, lo, n):
        col = pl.multiple_of((zz * 4 + yy) * 128, 128)
        return wd.at[lo * 88 : (lo + n) * 88, pl.ds(col, 128)]

    def gather(g, piece):
        def put(n, zz, yy, lo, cnt, dev):
            p = piece(zz, yy, lo, cnt)
            remote(p, p, wg_s.at[g, n], wg_r.at[g, n], dev).start()

        def got(n, zz, yy, lo, cnt):
            p = piece(zz, yy, lo, cnt)
            remote(p, p, wg_s.at[g, n], wg_r.at[g, n], YR).wait_recv()

        def s0():
            put(0, z, y, 0, 4, YR)
            put(1, z, y, 0, 4, YL)
            put(2, z, y, 4, 4, ZR)
            put(3, z, y, 4, 4, ZL)

        def s0b():
            put(4, z, y, 0, 4, ZR)
            put(5, z, y, 0, 4, ZL)
            put(6, z, y, 4, 4, YR)
            put(7, z, y, 4, 4, YL)

        def s1():
            got(0, z, yl, 0, 4)
            put(8, z, yl, 0, 2, YR)
            got(1, z, yr, 0, 4)
            put(9, z, yr, 2, 2, YL)
            got(2, zl, y, 4, 4)
            put(10, zl, y, 4, 2, ZR)
            got(3, zr, y, 4, 4)
            put(11, zr, y, 6, 2, ZL)
            put(12, z, yl, 0, 4, ZR)
            put(13, z, yl, 0, 4, ZL)
            put(14, zl, y, 4, 4, YR)
            put(15, zl, y, 4, 4, YL)
            put(16, z, yr, 0, 4, ZR)
            put(17, z, yr, 0, 4, ZL)
            put(18, zr, y, 4, 4, YR)
            put(19, zr, y, 4, 4, YL)

        def s2():
            got(8, z, yo, 0, 2)
            got(9, z, yo, 2, 2)
            got(10, zo, y, 4, 2)
            got(11, zo, y, 6, 2)
            put(20, z, yo, 0, 4, ZR)
            put(21, z, yo, 0, 4, ZL)
            put(22, zo, y, 4, 4, YR)
            put(23, zo, y, 4, 4, YL)

        def s3(m):
            n = (4, 12, 16, 20)[m]
            w = 24 + 4 * m
            ym, zm = (y, yl, yr, yo)[m], (z, zl, zr, zo)[m]
            nb = n + 2
            got(n, zl, ym, 0, 4)
            put(w, zl, ym, 0, 2, ZR)
            got(n + 1, zr, ym, 0, 4)
            put(w + 1, zr, ym, 2, 2, ZL)
            got(nb, zm, yl, 4, 4)
            put(w + 2, zm, yl, 4, 2, YR)
            got(nb + 1, zm, yr, 4, 4)
            put(w + 3, zm, yr, 6, 2, YL)

        def s4():
            for m in range(4):
                w = 24 + 4 * m
                ym, zm = (y, yl, yr, yo)[m], (z, zl, zr, zo)[m]
                got(w, zo, ym, 0, 2)
                got(w + 1, zo, ym, 2, 2)
                got(w + 2, zm, yo, 4, 2)
                got(w + 3, zm, yo, 6, 2)

        def drain():
            for n in range(40):
                cnt = 2 if 8 <= n < 12 or n >= 24 else 4
                p = piece(z, y, 0, cnt)
                remote(p, p, wg_s.at[g, n], wg_r.at[g, n], YR).wait_send()

        return s0, s0b, s1, s2, s3, s4, drain

    u0, u0b, u1, u2, u3, u4, udrain = gather(0, up_piece)
    n0, n0b, n1, n2, n3, n4, ndrain = gather(1, dn_piece)

    lsc[...] = jnp.zeros((8, 256), F32)
    for b in range(4):
        lsc[b : b + 1, 0:128] = log_ref[2 * b : 2 * b + 1, :]
        lsc[b : b + 1, 128:256] = log_ref[2 * b + 1 : 2 * b + 2, :]
    ri = lax.broadcasted_iota(jnp.int32, (BLK, BLK), 0)
    ci = lax.broadcasted_iota(jnp.int32, (BLK, BLK), 1)
    causal = ri >= ci
    tri = jnp.where(causal, 1.0, 0.0).astype(F32)
    logs = lsc[...]
    crow[...] = lax.dot_general(logs, tri, NT, precision=HIGH, preferred_element_type=F32)
    ccol[...] = lax.dot_general(tri, logs, NT, precision=HIGH, preferred_element_type=F32)

    wd[FF:FFP, :] = jnp.zeros((FFP - FF, 2048), BF16)

    for i in range(4):
        loads[i].wait()
    for n in range(11):
        tile = ust[n * 128 : (n + 1) * 128, :].astype(F32)
        wu[me, :, n * 128 : (n + 1) * 128] = tile.T.astype(BF16)
    pl.semaphore_wait(barrier, NSP + 2)
    u0()
    u0b()

    base = tb_ref[me]

    def turned(ref, b):
        ci_, si_ = ti_ref[0], ti_ref[1]
        cb_, sb_ = base[b : b + 1, :], base[4 + b : 5 + b, :]
        cos = cb_ * ci_ - sb_ * si_
        sin = sb_ * ci_ + cb_ * si_
        front = ref[b * BLK : (b + 1) * BLK, 0:128].astype(F32)
        second = ref[b * BLK : (b + 1) * BLK, 128:256].astype(F32)
        return front * cos - second * sin, front * sin + second * cos

    loads[5].wait()
    loads[6].wait()
    decay = jnp.ones((1, 1), F32)
    for b in range(4):
        front, second = turned(kv, b)
        front = (front * 0.0625).astype(BF16)
        second = (second * 0.0625).astype(BF16)
        kr[b, :, 0:128] = front
        kr[b, :, 128:256] = second
        total = crow[b : b + 1, 255:256]
        to_end = jnp.exp(total - ccol[:, b : b + 1])
        faded = jnp.concatenate([front, second], axis=1).astype(F32) * to_end
        state = lax.dot_general(
            faded.astype(BF16), vv[b * BLK : (b + 1) * BLK, :], TN, preferred_element_type=F32
        )
        step = jnp.exp(total)
        dpre[b] = jnp.broadcast_to(decay, (8, 128))
        decay = decay * step
        if b == 0:
            loc[b] = jnp.zeros((BLK, 512), F32)
            loc[b + 1] = state
        else:
            loc[b + 1] = step * loc[b] + state

    hi = decay.astype(BF16)
    mid = (decay - hi.astype(F32)).astype(BF16)
    low = (decay - hi.astype(F32) - mid.astype(F32)).astype(BF16)
    row = lax.broadcasted_iota(jnp.int32, (16, 128), 0)
    tag = jnp.where(
        row == 0,
        hi.astype(F32),
        jnp.where(row == 1, mid.astype(F32), jnp.where(row == 2, low.astype(F32), 0.0)),
    ).astype(BF16)
    for j in range(NSP):
        ssend[j, :, 0:512] = loc[4, j * 16 : (j + 1) * 16, :].astype(BF16)
        ssend[j, :, 512:640] = tag
    srecv[me] = ssend[me]

    def scatter(i, carry):
        j, dev = sp_peer(i)
        remote(ssend.at[j], srecv.at[me], ss_s.at[j], ss_r.at[me], dev).start()
        return carry

    lax.fori_loop(1, NSP, scatter, 0)
    u1()

    loads[7].wait()
    for b in range(4):
        front, second = turned(qv, b)
        qr = jnp.concatenate([front, second], axis=1).astype(BF16)
        column = ccol[:, b : b + 1]
        sq[b] = (qr.astype(F32) * jnp.exp(column)).astype(BF16)
        scores = lax.dot_general(qr, kr[b], NT, preferred_element_type=F32)
        gap = column - crow[b : b + 1, :]
        weight = jnp.where(causal, jnp.exp(jnp.where(causal, gap, 0.0)), 0.0)
        within[b] = jnp.dot(
            (scores * weight).astype(BF16),
            vv[b * BLK : (b + 1) * BLK, :],
            preferred_element_type=F32,
        )

    def scattered(i, carry):
        j, dev = sp_peer(i)
        remote(ssend.at[j], srecv.at[j], ss_s.at[j], ss_r.at[j], dev).wait_recv()
        return carry

    lax.fori_loop(1, NSP, scattered, 0)
    acc = jnp.zeros((16, 512), F32)
    for d in range(NSP):
        rsend[d] = acc.astype(BF16)
        if d < NSP - 1:
            tags = srecv[d, :, 512:640].astype(F32)
            factor = tags[0:1, 0:1] + tags[1:2, 0:1] + tags[2:3, 0:1]
            acc = factor * acc + srecv[d, :, 0:512].astype(F32)
    inc[me] = rsend[me]

    def give_back(i, carry):
        j, dev = sp_peer(i)
        remote(rsend.at[j], inc.at[me], rs_s.at[j], rs_r.at[me], dev).start()
        return carry

    lax.fori_loop(1, NSP, give_back, 0)
    u2()
    u3(0)

    def given(i, carry):
        j, dev = sp_peer(i)
        remote(rsend.at[j], inc.at[j], rs_s.at[j], rs_r.at[j], dev).wait_recv()
        return carry

    lax.fori_loop(1, NSP, given, 0)

    order = (xo, xr, xl, x)

    def reduce_scatter(s, compute, polls):
        def pair(j):
            return remote(
                part.at[s, j, 1 - c], d2.at[s, j], d2_s.at[s, j], d2_r.at[s, j], SIB
            )

        def merged(j, lo, hi, extra=None):
            def rows(i, carry):
                r = pl.ds(pl.multiple_of(i * 32, 32), 32)
                v = part[s, j, c, r, lo:hi].astype(F32) + d2[s, j, r, lo:hi].astype(F32)
                if extra is not None:
                    v = v + extra[s, r, :].astype(F32)
                cb[s, j, r, lo:hi] = v.astype(BF16)
                return carry

            lax.fori_loop(0, 4, rows, 0)

        def across(n, src, dst, dev):
            return remote(src, dst, x_s.at[s, n], x_r.at[s, n], dev)

        L, R = slice(0, 1024), slice(1024, 2048)
        a_out = across(0, cb.at[s, 0, :, L], ra.at[s], XR)
        b_out = across(1, cb.at[s, 0, :, R], rb.at[s], XL)
        r_late = across(2, cb.at[s, 1, :, L], rl.at[s, :, L], XR)
        r_soon = across(3, cb.at[s, 1, :, R], rl.at[s, :, R], XR)
        l_soon = across(4, cb.at[s, 2, :, L], rr.at[s, :, L], XL)
        l_late = across(5, cb.at[s, 2, :, R], rr.at[s, :, R], XL)

        compute(0, order[0])
        pair(0).start()
        polls[0]()
        compute(1, order[1])
        pair(1).start()
        pair(0).wait_recv()
        merged(0, 0, 1024)
        a_out.start()
        merged(0, 1024, 2048)
        b_out.start()
        polls[1]()
        compute(2, order[2])
        pair(2).start()
        pair(1).wait_recv()
        merged(1, 1024, 2048)
        r_soon.start()
        polls[2]()
        compute(3, order[3])
        pair(3).start()
        pair(2).wait_recv()
        merged(2, 0, 1024)
        l_soon.start()
        a_out.wait_recv()
        merged(1, 0, 1024, ra)
        r_late.start()
        b_out.wait_recv()
        merged(2, 1024, 2048, rb)
        l_late.start()
        polls[3]()
        pair(3).wait_recv()
        for op in (r_soon, l_soon, r_late, l_late):
            op.wait_recv()

        def drain():
            for j in range(4):
                pair(j).wait_send()
            for op in (a_out, b_out, r_late, r_soon, l_soon, l_late):
                op.wait_send()

        return drain

    def summed(s, r):
        v = part[s, 3, c, r, :].astype(F32) + d2[s, 3, r, :].astype(F32)
        return v + rl[s, r, :].astype(F32) + rr[s, r, :].astype(F32)

    def normed(v, i):
        mean = jnp.mean(v, axis=-1, keepdims=True)
        v = v - mean
        var = jnp.mean(v * v, axis=-1, keepdims=True)
        return v * lax.rsqrt(var + EPS) * gain_ref[i : i + 1, :] + bias_ref[i : i + 1, :]

    for i in (8, 9):
        loads[i].wait()

    def attend(j, b):
        rows = pl.ds(pl.multiple_of(b * BLK, BLK), BLK)
        state = dpre[b][0:1, 0:1] * inc[...].reshape(BLK, 512).astype(F32) + loc[b]
        mixed = within[b] + jnp.dot(sq[b], state.astype(BF16), preferred_element_type=F32)
        mean = jnp.mean(mixed, axis=-1, keepdims=True)
        mixed = mixed - mean
        var = jnp.mean(mixed * mixed, axis=-1, keepdims=True)
        mixed = mixed * lax.rsqrt(var + EPS)
        gate = gv[rows, :].astype(F32)
        gr[...] = (gate * jax.nn.sigmoid(gate) * mixed).astype(BF16)

        def tile(n, carry):
            cols = pl.ds(pl.multiple_of(n * 512, 512), 512)
            p = jnp.dot(gr[...], owv[:, cols], preferred_element_type=F32)
            part[0, j, :, :, cols] = p.astype(BF16).reshape(2, 128, 512)
            return carry

        lax.fori_loop(0, 4, tile, 0)

    def poll_w(*fs):
        def run():
            for f in fs:
                f()

        return run

    loads[4].wait()
    drain0 = reduce_scatter(
        0,
        attend,
        (
            poll_w(functools.partial(u3, 1)),
            poll_w(functools.partial(u3, 2)),
            poll_w(functools.partial(u3, 3), n0, n0b),
            poll_w(u4, n1),
        ),
    )
    loads[10].wait()

    def first_norm(i, carry):
        r = pl.ds(pl.multiple_of(i * 16, 16), 16)
        v = ALPHA * rv[r, :].astype(F32) + summed(0, r)
        xb[t, r, :] = normed(v, 0).astype(BF16)
        return carry

    lax.fori_loop(0, 8, first_norm, 0)

    tl, tr, to = xl * 2 + c, xr * 2 + c, xo * 2 + c
    R0, R1, RA = slice(0, 64), slice(64, 128), slice(0, 128)

    def ag(n, dev_t, rows, dev):
        p = xb.at[dev_t, rows, :]
        return remote(p, p, ag_s.at[n], ag_r.at[n], dev)

    sends = []

    def go(n, dev_t, rows, dev):
        op = ag(n, dev_t, rows, dev)
        op.start()
        sends.append(op)

    def arrived(n, dev_t, rows):
        ag(n, dev_t, rows, SIB).wait_recv()

    go(1, t, R0, XR)
    go(3, t, R1, XL)
    go(0, t, RA, SIB)
    go(2, t, R1, XR)
    go(4, t, R0, XL)

    def up(b):
        rows = pl.ds(pl.multiple_of(16 + b * BLK, 16), BLK)

        def tile(n, carry):
            cols = pl.ds(pl.multiple_of(n * 256, 256), 256)
            lhs = xb[pl.ds(2 * b, 2)].reshape(BLK, 2048)
            w = wu[:, :, cols].reshape(2048, 256)
            ub[rows, cols] = jnp.dot(lhs, w, preferred_element_type=F32).astype(BF16)
            return carry

        lax.fori_loop(0, 5, tile, 0)
        lhs = xb[pl.ds(2 * b, 2)].reshape(BLK, 2048)
        w = wu[:, :, 1280:1408].reshape(2048, 128)
        ub[rows, 1280:1408] = jnp.dot(lhs, w, preferred_element_type=F32).astype(BF16)

    def halo_copy():
        nxt = lax.rem(me + 1, NSP)
        dev = {"z": lax.div(nxt, 4), "y": lax.rem(nxt, 4)}
        return remote(ub.at[1024:1040, :], halo, h_s.at[0], h_r.at[0], dev)

    def send_halo(when):
        @pl.when(jnp.logical_and(when, me < NSP - 1))
        def _():
            halo_copy().start()

    def take_halo(when):
        @pl.when(jnp.logical_and(when, me > 0))
        def _():
            halo_copy().wait_recv()
            ub[0:16, :] = halo[...]

    @pl.when(me == 0)
    def _():
        ub[0:16, :] = jnp.zeros((16, 1408), BF16)

    def conv(b):
        def three(block, half, n):
            w = taps_ref[3 * half : 3 * half + 3, n * 128 : (n + 1) * 128]
            shift = taps_ref[6 + half : 7 + half, n * 128 : (n + 1) * 128]
            v = shift + block[14:270] * w[0:1]
            v = v + block[15:271] * w[1:2]
            return v + block[16:272] * w[2:3]

        rows = pl.ds(pl.multiple_of(b * BLK, BLK), BLK)
        around = pl.ds(pl.multiple_of(b * BLK, BLK), BLK + 16)
        for n in range(6):
            if n < 5:
                g = ub[around, n * 128 : (n + 1) * 128].astype(F32)
                v = ub[around, 640 + n * 128 : 640 + (n + 1) * 128].astype(F32)
            else:
                g = ub[around, 1280:1408].astype(F32)
                v = pltpu.roll(g, 64, 1)
            a = jax.nn.gelu(three(g, 0, n)) * three(v, 1, n)
            if n == 5:
                lane = lax.broadcasted_iota(jnp.int32, (BLK, 128), 1)
                a = jnp.where(lane < 64, a, 0.0)
            act[rows, n * 128 : (n + 1) * 128] = a.astype(BF16)

    arrived(0, t + 1 - 2 * c, RA)
    n2()
    up(x)
    send_halo(x == 3)
    arrived(1, tl, R0)
    go(5, tl, R0, XR)
    arrived(3, tr, R1)
    go(6, tr, R1, XL)
    go(7, tl, R0, SIB)
    go(8, tr, R1, SIB)
    n3(0)
    n3(1)
    arrived(2, tl, R1)
    go(9, tl, R1, SIB)
    arrived(4, tr, R0)
    go(10, tr, R0, SIB)
    n3(2)
    n3(3)
    arrived(7, xl * 2 + 1 - c, R0)
    arrived(8, xr * 2 + 1 - c, R1)
    arrived(9, xl * 2 + 1 - c, R1)
    arrived(10, xr * 2 + 1 - c, R0)
    up(xr)
    send_halo(xr == 3)
    up(xl)
    send_halo(xl == 3)
    arrived(5, to, R0)
    go(11, to, R0, SIB)
    arrived(6, to, R1)
    go(12, to, R1, SIB)
    take_halo(x == 3)
    conv(xr)
    arrived(11, xo * 2 + 1 - c, R0)
    arrived(12, xo * 2 + 1 - c, R1)
    up(xo)
    send_halo(xo == 3)
    take_halo(x == 2)
    conv(xo)
    n4()

    def down(j, b):
        if j == 2:
            take_halo(x == 1)
            conv(xl)
        if j == 3:
            take_halo(x == 0)
            conv(x)
        rows = pl.ds(pl.multiple_of(b * BLK, BLK), BLK)

        def tile(n, carry):
            cols = pl.ds(pl.multiple_of(n * 512, 512), 512)
            p = jnp.dot(act[rows, :], wd[:, cols], preferred_element_type=F32)
            part[1, j, :, :, cols] = p.astype(BF16).reshape(2, 128, 512)
            return carry

        lax.fori_loop(0, 4, tile, 0)

    def nothing():
        pass

    drain1 = reduce_scatter(1, down, (nothing,) * 4)

    def last_norm(i, carry):
        r = pl.ds(pl.multiple_of(i * 16, 16), 16)
        v = ALPHA * xb[t, r, :].astype(F32) + summed(1, r)
        o_ref[r, :] = normed(v, 1).astype(BF16)
        return carry

    lax.fori_loop(0, 8, last_norm, 0)

    def drain_state(i, carry):
        j, dev = sp_peer(i)
        remote(ssend.at[j], srecv.at[me], ss_s.at[j], ss_r.at[me], dev).wait_send()
        remote(rsend.at[j], inc.at[me], rs_s.at[j], rs_r.at[me], dev).wait_send()
        return carry

    lax.fori_loop(1, NSP, drain_state, 0)
    udrain()
    ndrain()
    drain0()
    drain1()
    for op in sends:
        op.wait_send()

    @pl.when(me < NSP - 1)
    def _():
        halo_copy().wait_send()


def shards(q, k, v, g, logd, res, ow, gain, bias, ug, uv, cw, cbias, dw):
    ti, tb = position_tables()
    taps = jnp.concatenate([cw.reshape(6, FF), cbias], axis=0)
    taps = jnp.pad(taps, ((0, 0), (0, FFP - FF)))
    dma = pltpu.SemaphoreType.DMA
    vm = pl.BlockSpec(memory_space=pltpu.VMEM)
    hb = pl.BlockSpec(memory_space=pl.ANY)
    return pl.pallas_call(
        body,
        out_shape=jax.ShapeDtypeStruct((128, 2048), BF16),
        in_specs=[hb, hb, hb, hb, vm, hb, hb, vm, vm, hb, hb, vm, hb, vm, vm],
        out_specs=vm,
        scratch_shapes=[
            pltpu.VMEM((1024, 256), BF16),
            pltpu.VMEM((1024, 256), BF16),
            pltpu.VMEM((1024, 512), BF16),
            pltpu.VMEM((1024, 512), BF16),
            pltpu.VMEM((128, 2048), BF16),
            pltpu.VMEM((512, 2048), BF16),
            pltpu.VMEM((1408, 128), BF16),
            pltpu.VMEM((NSP, 128, 1408), BF16),
            pltpu.VMEM((FFP, 2048), BF16),
            pltpu.VMEM((8, 256), F32),
            pltpu.VMEM((8, 256), F32),
            pltpu.VMEM((256, 8), F32),
            pltpu.VMEM((4, 8, 128), F32),
            pltpu.VMEM((4, 256, 256), BF16),
            pltpu.VMEM((4, 256, 256), BF16),
            pltpu.VMEM((5, 256, 512), F32),
            pltpu.VMEM((4, 256, 512), F32),
            pltpu.VMEM((256, 512), BF16),
            pltpu.VMEM((NSP, 16, 640), BF16),
            pltpu.VMEM((NSP, 16, 640), BF16),
            pltpu.VMEM((NSP, 16, 512), BF16),
            pltpu.VMEM((NSP, 16, 512), BF16),
            pltpu.VMEM((2, 4, 2, 128, 2048), BF16),
            pltpu.VMEM((2, 4, 128, 2048), BF16),
            pltpu.VMEM((2, 3, 128, 2048), BF16),
            pltpu.VMEM((2, 128, 1024), BF16),
            pltpu.VMEM((2, 128, 1024), BF16),
            pltpu.VMEM((2, 128, 2048), BF16),
            pltpu.VMEM((2, 128, 2048), BF16),
            pltpu.VMEM((8, 128, 2048), BF16),
            pltpu.VMEM((1040, 1408), BF16),
            pltpu.VMEM((1024, FFP), BF16),
            pltpu.VMEM((16, 1408), BF16),
            dma((11,)),
            dma((NSP,)),
            dma((NSP,)),
            dma((NSP,)),
            dma((NSP,)),
            dma((2, 40)),
            dma((2, 40)),
            dma((2, 4)),
            dma((2, 4)),
            dma((2, 6)),
            dma((2, 6)),
            dma((13,)),
            dma((13,)),
            dma((1,)),
            dma((1,)),
        ],
        compiler_params=pltpu.CompilerParams(
            collective_id=0, has_side_effects=True, vmem_limit_bytes=62 * 1024 * 1024
        ),
        name="layer",
    )(q, k, v, g, logd.reshape(8, 128), res, ow, gain, bias, ug.T, uv.T, taps, dw, ti, tb)


def solution(mesh):
    torus = Mesh(mesh.devices.reshape(4, 4, 4, 2), ("z", "y", "x", "c"))
    sp, tp = ("z", "y"), ("x", "c")
    return jax.shard_map(
        shards,
        mesh=torus,
        in_specs=(
            P(sp, tp),
            P(sp, tp),
            P(sp, tp),
            P(sp, tp),
            P(sp, tp),
            P(sp, None),
            P(tp, None),
            P(),
            P(),
            P(sp, tp),
            P(sp, tp),
            P(None, None, tp),
            P(None, tp),
            P(tp, sp),
        ),
        out_specs=P(sp + tp, None),
        check_vma=False,
    )
```

```python
import functools

import jax
import jax.numpy as jnp
import numpy as np
from jax import lax
from jax.experimental import pallas as pl
from jax.experimental.pallas import tpu as pltpu
from jax.sharding import Mesh
from jax.sharding import PartitionSpec as P

F32 = jnp.float32
BF16 = jnp.bfloat16
HIGH = lax.Precision.HIGHEST
MESH = pl.DeviceIdType.MESH
ALPHA = 8.0**0.25
EPS = 1e-05
NSP = 16
BLK = 256
FF = 704
FFP = 768
NT = (((1,), (1,)), ((), ()))
TN = (((0,), (0,)), ((), ()))


def position_tables():
    freq = 10000.0 ** (-2.0 * np.arange(128, dtype=np.float64) / 256.0)
    inner = np.arange(BLK, dtype=np.float64)[:, None] * freq[None]
    start = np.arange(4 * NSP, dtype=np.float64)[:, None] * BLK * freq[None]
    ti = np.stack([np.cos(inner), np.sin(inner)]).astype(np.float32)
    tb = np.concatenate(
        [np.cos(start).reshape(NSP, 4, 128), np.sin(start).reshape(NSP, 4, 128)], axis=1
    ).astype(np.float32)
    return ti, tb


def body(
    q_h, k_h, v_h, g_h, log_h, res_h, ow_h, gain_h, bias_h, ug_h, uv_h, taps_h, shift_h, dw_h,
    ti_h, tb_h, o_ref,
    qv, kv, vv, gv, log_ref, rv, owv, gain_ref, bias_ref, ust, taps_ref, shift_ref, ti_ref, tb_ref,
    wu, wd,
    lsc, crow, ccol, dpre, kr, sq, loc, within, gr,
    ssend, srecv, rsend, inc,
    part, d2, cb, ra, rb, rl, rr,
    xb, ub, act, halo,
    in_sem, ss_s, ss_r, rs_s, rs_r, wg_s, wg_r, d2_s, d2_r, x_s, x_r, ag_s, ag_r, h_s, h_r,
):
    z, y, x, c = (lax.axis_index(a) for a in ("z", "y", "x", "c"))
    me = z * 4 + y
    t = x * 2 + c
    xr, xl, xo = lax.rem(x + 1, 4), lax.rem(x + 3, 4), lax.rem(x + 2, 4)

    def at(axis, value):
        return {axis: value}

    SIB = at("c", 1 - c)
    XR, XL = at("x", xr), at("x", xl)

    def remote(src, dst, ssem, rsem, dev):
        return pltpu.make_async_remote_copy(
            src_ref=src, dst_ref=dst, send_sem=ssem, recv_sem=rsem, device_id=dev,
            device_id_type=MESH,
        )

    loads = {
        "log": (log_h, log_ref),
        "k": (k_h, kv),
        "ti": (ti_h, ti_ref),
        "tb": (tb_h.at[me], tb_ref),
        "v": (v_h, vv),
        "ug": (ug_h.at[0:640], ust.at[0:640]),
        "uv": (uv_h.at[0:640], ust.at[640:1280]),
        "ug2": (ug_h.at[640:704], ust.at[1280:1344]),
        "uv2": (uv_h.at[640:704], ust.at[1344:1408]),
        "q": (q_h, qv),
        "g": (g_h, gv),
        "ow": (ow_h, owv),
        "dw": (dw_h, wd.at[0:FF, pl.ds(pl.multiple_of(me * 128, 128), 128)]),
        "res": (res_h.at[pl.ds(pl.multiple_of(t * 128, 128), 128)], rv),
        "gain": (gain_h, gain_ref),
        "bias": (bias_h, bias_ref),
        "taps": (taps_h, taps_ref),
        "shift": (shift_h, shift_ref),
    }
    loads = {
        name: pltpu.make_async_copy(src, dst, in_sem.at[i])
        for i, (name, (src, dst)) in enumerate(loads.items())
    }
    for load in loads.values():
        load.start()

    def loaded(*names):
        for name in names:
            loads[name].wait()

    barrier = pltpu.get_barrier_semaphore()

    def sp_peer(i):
        j = lax.rem(me + i, NSP)
        return j, {"z": lax.div(j, 4), "y": lax.rem(j, 4)}

    def greet(i, carry):
        _, dev = sp_peer(i)
        pl.semaphore_signal(barrier, inc=1, device_id=dev, device_id_type=MESH)
        return carry

    lax.fori_loop(1, NSP, greet, 0)
    for dev in (SIB, XR, XL):
        pl.semaphore_signal(barrier, inc=1, device_id=dev, device_id_type=MESH)

    yr, yl, yo = lax.rem(y + 1, 4), lax.rem(y + 3, 4), lax.rem(y + 2, 4)
    zr, zl, zo = lax.rem(z + 1, 4), lax.rem(z + 3, 4), lax.rem(z + 2, 4)
    YR, YL, ZR, ZL = at("y", yr), at("y", yl), at("z", zr), at("z", zl)

    def up_piece(zz, yy, lo, n):
        return wu.at[zz * 4 + yy, lo * 16 : (lo + n) * 16, :]

    def dn_piece(zz, yy, lo, n):
        col = pl.multiple_of((zz * 4 + yy) * 128, 128)
        return wd.at[lo * 88 : (lo + n) * 88, pl.ds(col, 128)]

    def gather(g, piece):
        def put(n, zz, yy, lo, cnt, dev):
            p = piece(zz, yy, lo, cnt)
            remote(p, p, wg_s.at[g, n], wg_r.at[g, n], dev).start()

        def got(n, zz, yy, lo, cnt):
            p = piece(zz, yy, lo, cnt)
            remote(p, p, wg_s.at[g, n], wg_r.at[g, n], YR).wait_recv()

        def s0():
            put(0, z, y, 0, 4, YR)
            put(1, z, y, 0, 4, YL)
            put(2, z, y, 4, 4, ZR)
            put(3, z, y, 4, 4, ZL)

        def s0b():
            put(4, z, y, 0, 4, ZR)
            put(5, z, y, 0, 4, ZL)
            put(6, z, y, 4, 4, YR)
            put(7, z, y, 4, 4, YL)

        def s1():
            got(0, z, yl, 0, 4)
            put(8, z, yl, 0, 2, YR)
            got(1, z, yr, 0, 4)
            put(9, z, yr, 2, 2, YL)
            got(2, zl, y, 4, 4)
            put(10, zl, y, 4, 2, ZR)
            got(3, zr, y, 4, 4)
            put(11, zr, y, 6, 2, ZL)
            put(12, z, yl, 0, 4, ZR)
            put(13, z, yl, 0, 4, ZL)
            put(14, zl, y, 4, 4, YR)
            put(15, zl, y, 4, 4, YL)
            put(16, z, yr, 0, 4, ZR)
            put(17, z, yr, 0, 4, ZL)
            put(18, zr, y, 4, 4, YR)
            put(19, zr, y, 4, 4, YL)

        def s2():
            got(8, z, yo, 0, 2)
            got(9, z, yo, 2, 2)
            got(10, zo, y, 4, 2)
            got(11, zo, y, 6, 2)
            put(20, z, yo, 0, 4, ZR)
            put(21, z, yo, 0, 4, ZL)
            put(22, zo, y, 4, 4, YR)
            put(23, zo, y, 4, 4, YL)

        def s3(m):
            n = (4, 12, 16, 20)[m]
            w = 24 + 4 * m
            ym, zm = (y, yl, yr, yo)[m], (z, zl, zr, zo)[m]
            nb = n + 2
            got(n, zl, ym, 0, 4)
            put(w, zl, ym, 0, 2, ZR)
            got(n + 1, zr, ym, 0, 4)
            put(w + 1, zr, ym, 2, 2, ZL)
            got(nb, zm, yl, 4, 4)
            put(w + 2, zm, yl, 4, 2, YR)
            got(nb + 1, zm, yr, 4, 4)
            put(w + 3, zm, yr, 6, 2, YL)

        def s4():
            for m in range(4):
                w = 24 + 4 * m
                ym, zm = (y, yl, yr, yo)[m], (z, zl, zr, zo)[m]
                got(w, zo, ym, 0, 2)
                got(w + 1, zo, ym, 2, 2)
                got(w + 2, zm, yo, 4, 2)
                got(w + 3, zm, yo, 6, 2)

        def drain():
            for n in range(40):
                cnt = 2 if 8 <= n < 12 or n >= 24 else 4
                p = piece(z, y, 0, cnt)
                remote(p, p, wg_s.at[g, n], wg_r.at[g, n], YR).wait_send()

        return s0, s0b, s1, s2, s3, s4, drain

    u0, u0b, u1, u2, u3, u4, udrain = gather(0, up_piece)
    n0, n0b, n1, n2, n3, n4, ndrain = gather(1, dn_piece)

    ri = lax.broadcasted_iota(jnp.int32, (BLK, BLK), 0)
    ci = lax.broadcasted_iota(jnp.int32, (BLK, BLK), 1)
    causal = ri >= ci
    tri = jnp.where(causal, 1.0, 0.0).astype(F32)
    lsc[...] = jnp.zeros((8, 256), F32)
    loaded("log")
    for b in range(4):
        lsc[b : b + 1, 0:128] = log_ref[2 * b : 2 * b + 1, :]
        lsc[b : b + 1, 128:256] = log_ref[2 * b + 1 : 2 * b + 2, :]
    logs = lsc[...]
    crow[...] = lax.dot_general(logs, tri, NT, precision=HIGH, preferred_element_type=F32)
    ccol[...] = lax.dot_general(tri, logs, NT, precision=HIGH, preferred_element_type=F32)
    loaded("k", "ti", "tb", "v")
    base = tb_ref[...]

    def turned(ref, b):
        ci_, si_ = ti_ref[0], ti_ref[1]
        cb_, sb_ = base[b : b + 1, :], base[4 + b : 5 + b, :]
        cos = cb_ * ci_ - sb_ * si_
        sin = sb_ * ci_ + cb_ * si_
        front = ref[b * BLK : (b + 1) * BLK, 0:128].astype(F32)
        second = ref[b * BLK : (b + 1) * BLK, 128:256].astype(F32)
        return front * cos - second * sin, front * sin + second * cos

    decay = jnp.ones((1, 1), F32)
    for b in range(4):
        front, second = turned(kv, b)
        front = (front * 0.0625).astype(BF16)
        second = (second * 0.0625).astype(BF16)
        kr[b, :, 0:128] = front
        kr[b, :, 128:256] = second
        total = crow[b : b + 1, 255:256]
        to_end = jnp.exp(total - ccol[:, b : b + 1])
        faded = jnp.concatenate([front, second], axis=1).astype(F32) * to_end
        state = lax.dot_general(
            faded.astype(BF16), vv[b * BLK : (b + 1) * BLK, :], TN, preferred_element_type=F32
        )
        step = jnp.exp(total)
        dpre[b] = jnp.broadcast_to(decay, (8, 128))
        decay = decay * step
        if b == 0:
            loc[b] = jnp.zeros((BLK, 512), F32)
            loc[b + 1] = state
        else:
            loc[b + 1] = step * loc[b] + state

    hi = decay.astype(BF16)
    mid = (decay - hi.astype(F32)).astype(BF16)
    low = (decay - hi.astype(F32) - mid.astype(F32)).astype(BF16)
    row = lax.broadcasted_iota(jnp.int32, (16, 128), 0)
    tag = jnp.where(
        row == 0,
        hi.astype(F32),
        jnp.where(row == 1, mid.astype(F32), jnp.where(row == 2, low.astype(F32), 0.0)),
    ).astype(BF16)
    for j in range(NSP):
        ssend[j, :, 0:512] = loc[4, j * 16 : (j + 1) * 16, :].astype(BF16)
        ssend[j, :, 512:640] = tag

    pl.semaphore_wait(barrier, NSP + 2)

    def scatter(i, carry):
        j, dev = sp_peer(i)
        remote(ssend.at[j], srecv.at[me], ss_s.at[j], ss_r.at[me], dev).start()
        return carry

    lax.fori_loop(1, NSP, scatter, 0)
    srecv[me] = ssend[me]

    loaded("ug", "uv", "ug2", "uv2")
    for n in range(11):
        tile = ust[n * 128 : (n + 1) * 128, :].astype(F32)
        wu[me, :, n * 128 : (n + 1) * 128] = tile.T.astype(BF16)
    u0()

    loaded("q")
    for b in range(4):
        front, second = turned(qv, b)
        qr = jnp.concatenate([front, second], axis=1).astype(BF16)
        column = ccol[:, b : b + 1]
        sq[b] = (qr.astype(F32) * jnp.exp(column)).astype(BF16)
        scores = lax.dot_general(qr, kr[b], NT, preferred_element_type=F32)
        gap = column - crow[b : b + 1, :]
        weight = jnp.where(causal, jnp.exp(jnp.where(causal, gap, 0.0)), 0.0)
        within[b] = jnp.dot(
            (scores * weight).astype(BF16),
            vv[b * BLK : (b + 1) * BLK, :],
            preferred_element_type=F32,
        )
    wd[FF:FFP, :] = jnp.zeros((FFP - FF, 2048), BF16)
    act[:, FF:FFP] = jnp.zeros((1024, FFP - FF), BF16)

    def scattered(i, carry):
        j, dev = sp_peer(i)
        remote(ssend.at[j], srecv.at[j], ss_s.at[j], ss_r.at[j], dev).wait_recv()
        return carry

    lax.fori_loop(1, NSP, scattered, 0)
    acc = jnp.zeros((16, 512), F32)
    for d in range(NSP):
        rsend[d] = acc.astype(BF16)
        if d < NSP - 1:
            tags = srecv[d, :, 512:640].astype(F32)
            factor = tags[0:1, 0:1] + tags[1:2, 0:1] + tags[2:3, 0:1]
            acc = factor * acc + srecv[d, :, 0:512].astype(F32)
    inc[me] = rsend[me]

    def give_back(i, carry):
        j, dev = sp_peer(i)
        remote(rsend.at[j], inc.at[me], rs_s.at[j], rs_r.at[me], dev).start()
        return carry

    lax.fori_loop(1, NSP, give_back, 0)
    u0b()
    u1()

    def given(i, carry):
        j, dev = sp_peer(i)
        remote(rsend.at[j], inc.at[j], rs_s.at[j], rs_r.at[j], dev).wait_recv()
        return carry

    lax.fori_loop(1, NSP, given, 0)

    order = (xo, xr, xl, x)

    def reduce_scatter(s, compute, polls):
        def pair(j):
            return remote(
                part.at[s, j, 1 - c], d2.at[s, j], d2_s.at[s, j], d2_r.at[s, j], SIB
            )

        def merged(j, lo, hi, extra=None):
            def rows(i, carry):
                r = pl.ds(pl.multiple_of(i * 32, 32), 32)
                v = part[s, j, c, r, lo:hi].astype(F32) + d2[s, j, r, lo:hi].astype(F32)
                if extra is not None:
                    v = v + extra[s, r, :].astype(F32)
                cb[s, j, r, lo:hi] = v.astype(BF16)
                return carry

            lax.fori_loop(0, 4, rows, 0)

        def across(n, src, dst, dev):
            return remote(src, dst, x_s.at[s, n], x_r.at[s, n], dev)

        L, R = slice(0, 1024), slice(1024, 2048)
        a_out = across(0, cb.at[s, 0, :, L], ra.at[s], XR)
        b_out = across(1, cb.at[s, 0, :, R], rb.at[s], XL)
        r_late = across(2, cb.at[s, 1, :, L], rl.at[s, :, L], XR)
        r_soon = across(3, cb.at[s, 1, :, R], rl.at[s, :, R], XR)
        l_soon = across(4, cb.at[s, 2, :, L], rr.at[s, :, L], XL)
        l_late = across(5, cb.at[s, 2, :, R], rr.at[s, :, R], XL)

        compute(0, order[0])
        pair(0).start()
        compute(1, order[1])
        pair(1).start()
        pair(0).wait_recv()
        merged(0, 0, 1024)
        a_out.start()
        merged(0, 1024, 2048)
        b_out.start()
        compute(2, order[2])
        pair(2).start()
        pair(1).wait_recv()
        merged(1, 1024, 2048)
        r_soon.start()
        compute(3, order[3])
        pair(3).start()
        pair(2).wait_recv()
        merged(2, 0, 1024)
        l_soon.start()
        polls[0]()
        a_out.wait_recv()
        merged(1, 0, 1024, ra)
        r_late.start()
        b_out.wait_recv()
        merged(2, 1024, 2048, rb)
        l_late.start()
        polls[1]()
        pair(3).wait_recv()
        for op in (r_soon, l_soon, r_late, l_late):
            op.wait_recv()

        def drain():
            for j in range(4):
                pair(j).wait_send()
            for op in (a_out, b_out, r_late, r_soon, l_soon, l_late):
                op.wait_send()

        return drain

    def summed(s, r):
        v = part[s, 3, c, r, :].astype(F32) + d2[s, 3, r, :].astype(F32)
        return v + rl[s, r, :].astype(F32) + rr[s, r, :].astype(F32)

    def normed(v, i):
        mean = jnp.mean(v, axis=-1, keepdims=True)
        v = v - mean
        var = jnp.mean(v * v, axis=-1, keepdims=True)
        return v * lax.rsqrt(var + EPS) * gain_ref[i : i + 1, :] + bias_ref[i : i + 1, :]

    loaded("g", "ow")

    def attend(j, b):
        rows = pl.ds(pl.multiple_of(b * BLK, BLK), BLK)
        state = dpre[b][0:1, 0:1] * inc[...].reshape(BLK, 512).astype(F32) + loc[b]
        mixed = within[b] + jnp.dot(sq[b], state.astype(BF16), preferred_element_type=F32)
        mean = jnp.mean(mixed, axis=-1, keepdims=True)
        mixed = mixed - mean
        var = jnp.mean(mixed * mixed, axis=-1, keepdims=True)
        mixed = mixed * lax.rsqrt(var + EPS)
        gate = gv[rows, :].astype(F32)
        gr[...] = (gate * jax.nn.sigmoid(gate) * mixed).astype(BF16)

        def tile(n, carry):
            cols = pl.ds(pl.multiple_of(n * 512, 512), 512)
            p = jnp.dot(gr[...], owv[:, cols], preferred_element_type=F32)
            part[0, j, :, :, cols] = p.astype(BF16).reshape(2, 128, 512)
            return carry

        lax.fori_loop(0, 4, tile, 0)

    def early():
        u2()
        u3(0)
        u3(1)

    def later():
        u3(2)
        u3(3)
        loaded("dw")
        n0()
        n0b()

    drain0 = reduce_scatter(0, attend, (early, later))
    loaded("res", "gain", "bias")

    def first_norm(i, carry):
        r = pl.ds(pl.multiple_of(i * 32, 32), 32)
        v = ALPHA * rv[r, :].astype(F32) + summed(0, r)
        xb[t, r, :] = normed(v, 0).astype(BF16)
        return carry

    tl, tr, to = xl * 2 + c, xr * 2 + c, xo * 2 + c
    R0, R1, RA = slice(0, 64), slice(64, 128), slice(0, 128)

    def ag(n, dev_t, rows, dev):
        p = xb.at[dev_t, rows, :]
        return remote(p, p, ag_s.at[n], ag_r.at[n], dev)

    sends = []

    def go(n, dev_t, rows, dev):
        op = ag(n, dev_t, rows, dev)
        op.start()
        sends.append(op)

    def arrived(n, dev_t, rows):
        ag(n, dev_t, rows, SIB).wait_recv()

    lax.fori_loop(0, 2, first_norm, 0)
    go(1, t, R0, XR)
    lax.fori_loop(2, 4, first_norm, 0)
    go(3, t, R1, XL)
    go(0, t, RA, SIB)
    go(2, t, R1, XR)
    go(4, t, R0, XL)

    def up(b):
        rows = pl.ds(pl.multiple_of(16 + b * BLK, 16), BLK)

        def tile(n, carry):
            cols = pl.ds(pl.multiple_of(n * 256, 256), 256)
            lhs = xb[pl.ds(2 * b, 2)].reshape(BLK, 2048)
            w = wu[:, :, cols].reshape(2048, 256)
            ub[rows, cols] = jnp.dot(lhs, w, preferred_element_type=F32).astype(BF16)
            return carry

        lax.fori_loop(0, 5, tile, 0)
        lhs = xb[pl.ds(2 * b, 2)].reshape(BLK, 2048)
        w = wu[:, :, 1280:1408].reshape(2048, 128)
        ub[rows, 1280:1408] = jnp.dot(lhs, w, preferred_element_type=F32).astype(BF16)

    def halo_copy():
        nxt = lax.rem(me + 1, NSP)
        dev = {"z": lax.div(nxt, 4), "y": lax.rem(nxt, 4)}
        return remote(ub.at[1024:1040, :], halo, h_s.at[0], h_r.at[0], dev)

    def send_halo(when):
        @pl.when(jnp.logical_and(when, me < NSP - 1))
        def _():
            halo_copy().start()

    def take_halo(when):
        @pl.when(jnp.logical_and(when, me > 0))
        def _():
            halo_copy().wait_recv()
            ub[0:16, :] = halo[...]

    @pl.when(me == 0)
    def _():
        ub[0:16, :] = jnp.zeros((16, 1408), BF16)

    def conv(b):
        def three(block, half, lanes):
            v = shift_ref[half : half + 1, lanes] + block[14:270] * taps_ref[0, half : half + 1, lanes]
            v = v + block[15:271] * taps_ref[1, half : half + 1, lanes]
            return v + block[16:272] * taps_ref[2, half : half + 1, lanes]

        rows = pl.ds(pl.multiple_of(b * BLK, BLK), BLK)
        around = pl.ds(pl.multiple_of(b * BLK, BLK), BLK + 16)
        for n in range(6):
            if n < 5:
                lanes = slice(n * 128, (n + 1) * 128)
                g = ub[around, lanes].astype(F32)
                v = ub[around, 640 + n * 128 : 640 + (n + 1) * 128].astype(F32)
            else:
                lanes = slice(640, FF)
                both = ub[around, 1280:1408].astype(F32)
                g, v = both[:, 0:64], pltpu.roll(both, 64, 1)[:, 0:64]
            a = jax.nn.gelu(three(g, 0, lanes)) * three(v, 1, lanes)
            act[rows, lanes] = a.astype(BF16)

    arrived(0, t + 1 - 2 * c, RA)
    u4()
    n1()
    loaded("taps", "shift")
    up(x)
    send_halo(x == 3)
    arrived(1, tl, R0)
    go(5, tl, R0, XR)
    arrived(3, tr, R1)
    go(6, tr, R1, XL)
    go(7, tl, R0, SIB)
    go(8, tr, R1, SIB)
    n2()
    n3(0)
    n3(1)
    arrived(2, tl, R1)
    go(9, tl, R1, SIB)
    arrived(4, tr, R0)
    go(10, tr, R0, SIB)
    n3(2)
    n3(3)
    arrived(7, xl * 2 + 1 - c, R0)
    arrived(8, xr * 2 + 1 - c, R1)
    arrived(9, xl * 2 + 1 - c, R1)
    arrived(10, xr * 2 + 1 - c, R0)
    up(xr)
    send_halo(xr == 3)
    up(xl)
    send_halo(xl == 3)
    arrived(5, to, R0)
    go(11, to, R0, SIB)
    arrived(6, to, R1)
    go(12, to, R1, SIB)
    take_halo(x == 3)
    conv(xr)
    arrived(11, xo * 2 + 1 - c, R0)
    arrived(12, xo * 2 + 1 - c, R1)
    up(xo)
    send_halo(xo == 3)
    take_halo(x == 2)
    conv(xo)
    n4()

    def down(j, b):
        if j == 2:
            take_halo(x == 1)
            conv(xl)
        if j == 3:
            take_halo(x == 0)
            conv(x)
        rows = pl.ds(pl.multiple_of(b * BLK, BLK), BLK)

        def tile(n, carry):
            cols = pl.ds(pl.multiple_of(n * 512, 512), 512)
            p = jnp.dot(act[rows, :], wd[:, cols], preferred_element_type=F32)
            part[1, j, :, :, cols] = p.astype(BF16).reshape(2, 128, 512)
            return carry

        lax.fori_loop(0, 4, tile, 0)

    def nothing():
        pass

    drain1 = reduce_scatter(1, down, (nothing, nothing))

    def last_norm(i, carry):
        r = pl.ds(pl.multiple_of(i * 32, 32), 32)
        v = ALPHA * xb[t, r, :].astype(F32) + summed(1, r)
        o_ref[r, :] = normed(v, 1).astype(BF16)
        return carry

    lax.fori_loop(0, 4, last_norm, 0)

    def drain_state(i, carry):
        j, dev = sp_peer(i)
        remote(ssend.at[j], srecv.at[me], ss_s.at[j], ss_r.at[me], dev).wait_send()
        remote(rsend.at[j], inc.at[me], rs_s.at[j], rs_r.at[me], dev).wait_send()
        return carry

    lax.fori_loop(1, NSP, drain_state, 0)
    udrain()
    ndrain()
    drain0()
    drain1()
    for op in sends:
        op.wait_send()

    @pl.when(me < NSP - 1)
    def _():
        halo_copy().wait_send()


def shards(q, k, v, g, logd, res, ow, gain, bias, ug, uv, cw, cbias, dw):
    ti, tb = position_tables()
    dma = pltpu.SemaphoreType.DMA
    vm = pl.BlockSpec(memory_space=pltpu.VMEM)
    hb = pl.BlockSpec(memory_space=pl.ANY)
    return pl.pallas_call(
        body,
        out_shape=jax.ShapeDtypeStruct((128, 2048), BF16),
        in_specs=[hb] * 16,
        out_specs=vm,
        scratch_shapes=[
            pltpu.VMEM((1024, 256), BF16),
            pltpu.VMEM((1024, 256), BF16),
            pltpu.VMEM((1024, 512), BF16),
            pltpu.VMEM((1024, 512), BF16),
            pltpu.VMEM((8, 128), F32),
            pltpu.VMEM((128, 2048), BF16),
            pltpu.VMEM((512, 2048), BF16),
            pltpu.VMEM((2, 2048), F32),
            pltpu.VMEM((2, 2048), F32),
            pltpu.VMEM((1408, 128), BF16),
            pltpu.VMEM((3, 2, FF), F32),
            pltpu.VMEM((2, FF), F32),
            pltpu.VMEM((2, BLK, 128), F32),
            pltpu.VMEM((8, 128), F32),
            pltpu.VMEM((NSP, 128, 1408), BF16),
            pltpu.VMEM((FFP, 2048), BF16),
            pltpu.VMEM((8, 256), F32),
            pltpu.VMEM((8, 256), F32),
            pltpu.VMEM((256, 8), F32),
            pltpu.VMEM((4, 8, 128), F32),
            pltpu.VMEM((4, 256, 256), BF16),
            pltpu.VMEM((4, 256, 256), BF16),
            pltpu.VMEM((5, 256, 512), F32),
            pltpu.VMEM((4, 256, 512), F32),
            pltpu.VMEM((256, 512), BF16),
            pltpu.VMEM((NSP, 16, 640), BF16),
            pltpu.VMEM((NSP, 16, 640), BF16),
            pltpu.VMEM((NSP, 16, 512), BF16),
            pltpu.VMEM((NSP, 16, 512), BF16),
            pltpu.VMEM((2, 4, 2, 128, 2048), BF16),
            pltpu.VMEM((2, 4, 128, 2048), BF16),
            pltpu.VMEM((2, 3, 128, 2048), BF16),
            pltpu.VMEM((2, 128, 1024), BF16),
            pltpu.VMEM((2, 128, 1024), BF16),
            pltpu.VMEM((2, 128, 2048), BF16),
            pltpu.VMEM((2, 128, 2048), BF16),
            pltpu.VMEM((8, 128, 2048), BF16),
            pltpu.VMEM((1040, 1408), BF16),
            pltpu.VMEM((1024, FFP), BF16),
            pltpu.VMEM((16, 1408), BF16),
            dma((18,)),
            dma((NSP,)),
            dma((NSP,)),
            dma((NSP,)),
            dma((NSP,)),
            dma((2, 40)),
            dma((2, 40)),
            dma((2, 4)),
            dma((2, 4)),
            dma((2, 6)),
            dma((2, 6)),
            dma((13,)),
            dma((13,)),
            dma((1,)),
            dma((1,)),
        ],
        compiler_params=pltpu.CompilerParams(
            collective_id=0, has_side_effects=True, vmem_limit_bytes=62 * 1024 * 1024
        ),
        name="layer",
    )(
        q, k, v, g, logd.reshape(8, 128), res, ow, gain, bias, ug.T, uv.T,
        cw.transpose(1, 0, 2), cbias, dw, ti, tb,
    )


def solution(mesh):
    torus = Mesh(mesh.devices.reshape(4, 4, 4, 2), ("z", "y", "x", "c"))
    sp, tp = ("z", "y"), ("x", "c")
    return jax.shard_map(
        shards,
        mesh=torus,
        in_specs=(
            P(sp, tp),
            P(sp, tp),
            P(sp, tp),
            P(sp, tp),
            P(sp, tp),
            P(sp, None),
            P(tp, None),
            P(),
            P(),
            P(sp, tp),
            P(sp, tp),
            P(None, None, tp),
            P(None, tp),
            P(tp, sp),
        ),
        out_specs=P(sp + tp, None),
        check_vma=False,
    )
```

```python
import functools

import jax
import jax.numpy as jnp
import numpy as np
from jax import lax
from jax.experimental import pallas as pl
from jax.experimental.pallas import tpu as pltpu
from jax.sharding import Mesh
from jax.sharding import PartitionSpec as P

F32 = jnp.float32
BF16 = jnp.bfloat16
HIGH = lax.Precision.HIGHEST
MESH = pl.DeviceIdType.MESH
ALPHA = 8.0**0.25
EPS = 1e-05
NSP = 16
BLK = 256
FF = 704
FFP = 768
ROWS = (((64, 128), (0, 64)), ((80, 128), (0, 80)))
NT = (((1,), (1,)), ((), ()))
TN = (((0,), (0,)), ((), ()))


def position_tables():
    freq = 10000.0 ** (-2.0 * np.arange(128, dtype=np.float64) / 256.0)
    inner = np.arange(BLK, dtype=np.float64)[:, None] * freq[None]
    start = np.arange(4 * NSP, dtype=np.float64)[:, None] * BLK * freq[None]
    ti = np.stack([np.cos(inner), np.sin(inner)]).astype(np.float32)
    tb = np.concatenate(
        [np.cos(start).reshape(NSP, 4, 128), np.sin(start).reshape(NSP, 4, 128)], axis=1
    ).astype(np.float32)
    return ti, tb


def body(
    q_h, k_h, v_h, g_h, log_h, res_h, ow_h, gain_h, bias_h, ug_h, uv_h, taps_h, shift_h, dw_h,
    ti_h, tb_h, o_ref,
    qv, kv, vv, gv, log_ref, rv, owv, gain_ref, bias_ref, ust, taps_ref, shift_ref, ti_ref, tb_ref,
    wu, wd,
    lsc, crow, ccol, dpre, kr, sq, loc, within, gr,
    ssend, srecv, rsend, inc,
    part, d2, cb, ra, rb, rl, rr,
    xb, ub, act0, act1, halo, ov,
    in_sem, st_s, st_r, wg_s, wg_r, d2_s, d2_r, x_s, x_r, ag_s, ag_r, h_s, h_r, out_sem,
):
    z, y, x, c = (lax.axis_index(a) for a in ("z", "y", "x", "c"))
    me = z * 4 + y
    t = x * 2 + c
    xr, xl, xo = lax.rem(x + 1, 4), lax.rem(x + 3, 4), lax.rem(x + 2, 4)

    def at(axis, value):
        return {axis: value}

    SIB = at("c", 1 - c)
    XR, XL = at("x", xr), at("x", xl)

    def remote(src, dst, ssem, rsem, dev):
        return pltpu.make_async_remote_copy(
            src_ref=src, dst_ref=dst, send_sem=ssem, recv_sem=rsem, device_id=dev,
            device_id_type=MESH,
        )

    loads = {
        "log": (log_h, log_ref),
        "k": (k_h, kv),
        "ti": (ti_h, ti_ref),
        "tb": (tb_h.at[me], tb_ref),
        "v": (v_h, vv),
        "ug": (ug_h.at[0:640], ust.at[0:640]),
        "uv": (uv_h.at[0:640], ust.at[640:1280]),
        "ug2": (ug_h.at[640:704], ust.at[1280:1344]),
        "uv2": (uv_h.at[640:704], ust.at[1344:1408]),
        "q": (q_h, qv),
        "g": (g_h, gv),
        "ow": (ow_h, owv),
        "dw": (dw_h, wd.at[0:FF, pl.ds(pl.multiple_of(me * 128, 128), 128)]),
        "res": (res_h.at[pl.ds(pl.multiple_of(t * 128, 128), 128)], rv),
        "gain": (gain_h, gain_ref),
        "bias": (bias_h, bias_ref),
        "taps": (taps_h, taps_ref),
        "shift": (shift_h, shift_ref),
    }
    loads = {
        name: pltpu.make_async_copy(src, dst, in_sem.at[5 if i in (6, 7, 8) else i])
        for i, (name, (src, dst)) in enumerate(loads.items())
    }
    for load in loads.values():
        load.start()

    def loaded(*names):
        for name in names:
            loads[name].wait()

    barrier = pltpu.get_barrier_semaphore()

    def sp_peer(i):
        j = lax.rem(me + i, NSP)
        return j, {"z": lax.div(j, 4), "y": lax.rem(j, 4)}

    def greet(i, carry):
        _, dev = sp_peer(i)
        pl.semaphore_signal(barrier, inc=1, device_id=dev, device_id_type=MESH)
        return carry

    lax.fori_loop(1, NSP, greet, 0)
    for dev in (SIB, XR, XL):
        pl.semaphore_signal(barrier, inc=1, device_id=dev, device_id_type=MESH)

    yr, yl, yo = lax.rem(y + 1, 4), lax.rem(y + 3, 4), lax.rem(y + 2, 4)
    zr, zl, zo = lax.rem(z + 1, 4), lax.rem(z + 3, 4), lax.rem(z + 2, 4)
    YR, YL, ZR, ZL = at("y", yr), at("y", yl), at("z", zr), at("z", zl)

    def up_piece(zz, yy, lo, n):
        return wu.at[zz * 4 + yy, lo * 16 : (lo + n) * 16, :]

    def dn_piece(zz, yy, lo, n):
        col = pl.multiple_of((zz * 4 + yy) * 128, 128)
        return wd.at[lo * 88 : (lo + n) * 88, pl.ds(col, 128)]

    def gather(g, piece, bytes_of):
        def put(n, zz, yy, lo, cnt, dev):
            p = piece(zz, yy, lo, cnt)
            remote(p, p, wg_s.at[g], wg_r.at[g, n], dev).start()

        def got(n, shards):
            p = bytes_of(shards)
            remote(p, p, wg_s.at[g], wg_r.at[g, n], YR).wait_recv()

        def s0():
            put(0, z, y, 0, 4, YR)
            put(0, z, y, 0, 4, YL)
            put(0, z, y, 4, 4, ZR)
            put(0, z, y, 4, 4, ZL)

        def s0b():
            put(2, z, y, 0, 4, ZR)
            put(2, z, y, 0, 4, ZL)
            put(2, z, y, 4, 4, YR)
            put(2, z, y, 4, 4, YL)

        def s1():
            got(0, 2)
            put(1, z, yl, 0, 2, YR)
            put(1, z, yr, 2, 2, YL)
            put(1, zl, y, 4, 2, ZR)
            put(1, zr, y, 6, 2, ZL)
            put(3, z, yl, 0, 4, ZR)
            put(3, z, yl, 0, 4, ZL)
            put(3, zl, y, 4, 4, YR)
            put(3, zl, y, 4, 4, YL)
            put(4, z, yr, 0, 4, ZR)
            put(4, z, yr, 0, 4, ZL)
            put(4, zr, y, 4, 4, YR)
            put(4, zr, y, 4, 4, YL)

        def s2():
            got(1, 1)
            put(5, z, yo, 0, 4, ZR)
            put(5, z, yo, 0, 4, ZL)
            put(5, zo, y, 4, 4, YR)
            put(5, zo, y, 4, 4, YL)

        def s3(m):
            ym, zm = (y, yl, yr, yo)[m], (z, zl, zr, zo)[m]
            got(2 + m, 2)
            put(6, zl, ym, 0, 2, ZR)
            put(6, zr, ym, 2, 2, ZL)
            put(6, zm, yl, 4, 2, YR)
            put(6, zm, yr, 6, 2, YL)

        def s4():
            got(6, 4)

        def drain():
            p = bytes_of(15)
            remote(p, p, wg_s.at[g], wg_r.at[g, 0], YR).wait_send()

        return s0, s0b, s1, s2, s3, s4, drain

    u0, u0b, u1, u2, u3, u4, udrain = gather(0, up_piece, lambda n: wu.at[0:n])
    n0, n0b, n1, n2, n3, n4, ndrain = gather(1, dn_piece, lambda n: wd.at[0:FF, 0 : n * 128])

    ri = lax.broadcasted_iota(jnp.int32, (BLK, BLK), 0)
    ci = lax.broadcasted_iota(jnp.int32, (BLK, BLK), 1)
    causal = ri >= ci
    tri = jnp.where(causal, 1.0, 0.0).astype(F32)
    lsc[...] = jnp.zeros((8, 256), F32)
    loaded("log")
    for b in range(4):
        lsc[b : b + 1, 0:128] = log_ref[2 * b : 2 * b + 1, :]
        lsc[b : b + 1, 128:256] = log_ref[2 * b + 1 : 2 * b + 2, :]
    logs = lsc[...]
    crow[...] = lax.dot_general(logs, tri, NT, precision=HIGH, preferred_element_type=F32)
    ccol[...] = lax.dot_general(tri, logs, NT, precision=HIGH, preferred_element_type=F32)
    loaded("k", "ti", "tb", "v")
    base = tb_ref[...]

    def turned(ref, b):
        ci_, si_ = ti_ref[0], ti_ref[1]
        cb_, sb_ = base[b : b + 1, :], base[4 + b : 5 + b, :]
        cos = cb_ * ci_ - sb_ * si_
        sin = sb_ * ci_ + cb_ * si_
        front = ref[b * BLK : (b + 1) * BLK, 0:128].astype(F32)
        second = ref[b * BLK : (b + 1) * BLK, 128:256].astype(F32)
        return front * cos - second * sin, front * sin + second * cos

    decay = jnp.ones((1, 1), F32)
    for b in range(4):
        front, second = turned(kv, b)
        front = (front * 0.0625).astype(BF16)
        second = (second * 0.0625).astype(BF16)
        kr[b, :, 0:128] = front
        kr[b, :, 128:256] = second
        total = crow[b : b + 1, 255:256]
        to_end = jnp.exp(total - ccol[:, b : b + 1])
        faded = jnp.concatenate([front, second], axis=1).astype(F32) * to_end
        state = lax.dot_general(
            faded.astype(BF16), vv[b * BLK : (b + 1) * BLK, :], TN, preferred_element_type=F32
        )
        step = jnp.exp(total)
        dpre[b] = jnp.broadcast_to(decay, (8, 128))
        decay = decay * step
        if b == 0:
            loc[b] = jnp.zeros((BLK, 512), F32)
            loc[b + 1] = state
        else:
            loc[b + 1] = step * loc[b] + state

    hi = decay.astype(BF16)
    mid = (decay - hi.astype(F32)).astype(BF16)
    low = (decay - hi.astype(F32) - mid.astype(F32)).astype(BF16)
    row = lax.broadcasted_iota(jnp.int32, (16, 128), 0)
    tag = jnp.where(
        row == 0,
        hi.astype(F32),
        jnp.where(row == 1, mid.astype(F32), jnp.where(row == 2, low.astype(F32), 0.0)),
    ).astype(BF16)
    for j in range(NSP):
        ssend[j, :, 0:512] = loc[4, j * 16 : (j + 1) * 16, :].astype(BF16)
        ssend[j, :, 512:640] = tag

    pl.semaphore_wait(barrier, NSP + 2)

    def scatter(i, carry):
        j, dev = sp_peer(i)
        remote(ssend.at[j], srecv.at[me], st_s.at[0], st_r.at[0], dev).start()
        return carry

    lax.fori_loop(1, NSP, scatter, 0)
    srecv[me] = ssend[me]

    pltpu.make_async_copy(ust, ust, in_sem.at[5]).wait()
    for n in range(11):
        tile = ust[n * 128 : (n + 1) * 128, :].astype(F32)
        wu[me, :, n * 128 : (n + 1) * 128] = tile.T.astype(BF16)
    u0()

    loaded("q")
    for b in range(4):
        front, second = turned(qv, b)
        qr = jnp.concatenate([front, second], axis=1).astype(BF16)
        column = ccol[:, b : b + 1]
        sq[b] = (qr.astype(F32) * jnp.exp(column)).astype(BF16)
        scores = lax.dot_general(qr, kr[b], NT, preferred_element_type=F32)
        gap = column - crow[b : b + 1, :]
        weight = jnp.where(causal, jnp.exp(jnp.where(causal, gap, 0.0)), 0.0)
        within[b] = jnp.dot(
            (scores * weight).astype(BF16),
            vv[b * BLK : (b + 1) * BLK, :],
            preferred_element_type=F32,
        )
    wd[FF:FFP, :] = jnp.zeros((FFP - FF, 2048), BF16)
    act0[:, :, FF:FFP] = jnp.zeros((4, 96, FFP - FF), BF16)
    act1[:, :, FF:FFP] = jnp.zeros((4, 160, FFP - FF), BF16)

    fifteen = slice(0, NSP - 1)
    scattered = remote(ssend.at[fifteen], srecv.at[fifteen], st_s.at[0], st_r.at[0], YR)
    returned = remote(rsend.at[fifteen], inc.at[fifteen], st_s.at[1], st_r.at[1], YR)
    scattered.wait_recv()
    acc = jnp.zeros((16, 512), F32)
    for d in range(NSP):
        rsend[d] = acc.astype(BF16)
        if d < NSP - 1:
            tags = srecv[d, :, 512:640].astype(F32)
            factor = tags[0:1, 0:1] + tags[1:2, 0:1] + tags[2:3, 0:1]
            acc = factor * acc + srecv[d, :, 0:512].astype(F32)
    inc[me] = rsend[me]

    def give_back(i, carry):
        j, dev = sp_peer(i)
        remote(rsend.at[j], inc.at[me], st_s.at[1], st_r.at[1], dev).start()
        return carry

    lax.fori_loop(1, NSP, give_back, 0)
    u0b()
    u1()

    returned.wait_recv()

    order = (xo, xr, xl, x)
    L, R = slice(0, 1024), slice(1024, 2048)

    class Scatter:
        def __init__(self, s, h):
            self.s, self.h = s, h
            self.lo, self.hi = ROWS[s][h]
            rows = slice(self.lo, self.hi)

            def across(n, src, dst, dev):
                return remote(src, dst, x_s.at[s, h], x_r.at[s, h, n], dev)

            self.a_out = across(0, cb.at[s, 0, rows, L], ra.at[s, rows], XR)
            self.b_out = across(1, cb.at[s, 0, rows, R], rb.at[s, rows], XL)
            self.r_late = across(2, cb.at[s, 1, rows, L], rl.at[s, rows, L], XR)
            self.r_soon = across(2, cb.at[s, 1, rows, R], rl.at[s, rows, R], XR)
            self.l_soon = across(2, cb.at[s, 2, rows, L], rr.at[s, rows, L], XL)
            self.l_late = across(2, cb.at[s, 2, rows, R], rr.at[s, rows, R], XL)
            self.into = across(2, cb.at[s, 0:2, rows], d2.at[s, 0:2, rows], XR)
            self.away = across(2, cb.at[s, 0:3, rows], d2.at[s, 0:3, rows], XR)

        def pair(self, j):
            s, h, rows = self.s, self.h, slice(self.lo, self.hi)
            return remote(
                part.at[s, j, 1 - c, rows], d2.at[s, j, rows], d2_s.at[s, h], d2_r.at[s, h, j], SIB
            )

        def merged(self, j, cols, extra=None):
            s = self.s

            def step(i, carry):
                r = pl.ds(pl.multiple_of(self.lo + i * 16, 16), 16)
                v = part[s, j, c, r, cols].astype(F32) + d2[s, j, r, cols].astype(F32)
                if extra is not None:
                    v = v + extra[s, r, :].astype(F32)
                cb[s, j, r, cols] = v.astype(BF16)
                return carry

            lax.fori_loop(0, (self.hi - self.lo) // 16, step, 0)

        def far(self):
            self.pair(0).wait_recv()
            self.merged(0, L)
            self.a_out.start()
            self.merged(0, R)
            self.b_out.start()

        def soon_right(self):
            self.pair(1).wait_recv()
            self.merged(1, R)
            self.r_soon.start()

        def soon_left(self):
            self.pair(2).wait_recv()
            self.merged(2, L)
            self.l_soon.start()

        def late(self):
            self.a_out.wait_recv()
            self.merged(1, L, ra)
            self.r_late.start()
            self.b_out.wait_recv()
            self.merged(2, R, rb)
            self.l_late.start()

        def finish(self):
            self.pair(3).wait_recv()
            self.into.wait_recv()

        def each(self, step):
            def run(i, carry):
                step(pl.ds(pl.multiple_of(self.lo + i * 16, 16), 16))
                return carry

            lax.fori_loop(0, (self.hi - self.lo) // 16, run, 0)

        def drain(self):
            s, h, rows = self.s, self.h, slice(self.lo, self.hi)
            remote(
                d2.at[s, :, rows], d2.at[s, :, rows], d2_s.at[s, h], d2_r.at[s, h, 0], SIB
            ).wait_send()
            self.away.wait_send()

    def summed(s, r):
        v = part[s, 3, c, r, :].astype(F32) + d2[s, 3, r, :].astype(F32)
        return v + rl[s, r, :].astype(F32) + rr[s, r, :].astype(F32)

    def normed(v, i):
        mean = jnp.mean(v, axis=-1, keepdims=True)
        v = v - mean
        var = jnp.mean(v * v, axis=-1, keepdims=True)
        return v * lax.rsqrt(var + EPS) * gain_ref[i : i + 1, :] + bias_ref[i : i + 1, :]

    loaded("g", "ow")

    def attend(j, b):
        rows = pl.ds(pl.multiple_of(b * BLK, BLK), BLK)
        state = dpre[b][0:1, 0:1] * inc[...].reshape(BLK, 512).astype(F32) + loc[b]
        mixed = within[b] + jnp.dot(sq[b], state.astype(BF16), preferred_element_type=F32)
        mean = jnp.mean(mixed, axis=-1, keepdims=True)
        mixed = mixed - mean
        var = jnp.mean(mixed * mixed, axis=-1, keepdims=True)
        mixed = mixed * lax.rsqrt(var + EPS)
        gate = gv[rows, :].astype(F32)
        gr[...] = (gate * jax.nn.sigmoid(gate) * mixed).astype(BF16)

        def tile(n, carry):
            cols = pl.ds(pl.multiple_of(n * 512, 512), 512)
            p = jnp.dot(gr[...], owv[:, cols], preferred_element_type=F32)
            part[0, j, :, :, cols] = p.astype(BF16).reshape(2, 128, 512)
            return carry

        lax.fori_loop(0, 4, tile, 0)

    A = [Scatter(0, 0), Scatter(0, 1)]
    attend(0, order[0])
    for h in A:
        h.pair(0).start()
    attend(1, order[1])
    for h in A:
        h.pair(1).start()
    for h in A:
        h.far()
    attend(2, order[2])
    for h in A:
        h.pair(2).start()
    for h in A:
        h.soon_right()
    attend(3, order[3])
    for h in A:
        h.pair(3).start()
    for h in A:
        h.soon_left()
    u2()
    u3(0)
    u3(1)
    for h in A:
        h.late()
    u3(2)
    u3(3)
    loaded("dw")
    n0()
    n0b()
    loaded("res", "gain", "bias")

    def first_norm(r):
        v = ALPHA * rv[r, :].astype(F32) + summed(0, r)
        xb[t, r, :] = normed(v, 0).astype(BF16)

    tl, tr, to = xl * 2 + c, xr * 2 + c, xo * 2 + c
    W = slice(0, 2048)

    def ag(h, n, owner, cols, dev):
        lo, hi = ROWS[0][h]
        p = xb.at[owner, lo:hi, cols]
        return remote(p, p, ag_s.at[h], ag_r.at[h, n], dev)

    def go(h, n, owner, cols, dev):
        ag(h, n, owner, cols, dev).start()

    def several(h, n, owners):
        lo, hi = ROWS[0][h]
        p = xb.at[0:owners, lo:hi]
        return remote(p, p, ag_s.at[h], ag_r.at[h, n], SIB)

    def arrived(h, n, owner, cols):
        ag(h, n, owner, cols, SIB).wait_recv()

    def own_rows(h):
        go(h, 1, t, L, XR)
        go(h, 3, t, R, XL)
        go(h, 0, t, W, SIB)
        go(h, 2, t, R, XR)
        go(h, 4, t, L, XL)

    def pass_on(h):
        arrived(h, 1, tl, L)
        go(h, 5, tl, L, XR)
        arrived(h, 3, tr, R)
        go(h, 6, tr, R, XL)
        go(h, 7, tl, L, SIB)
        go(h, 7, tr, R, SIB)

    def pass_second(h):
        arrived(h, 2, tl, R)
        go(h, 7, tl, R, SIB)
        arrived(h, 4, tr, L)
        go(h, 7, tr, L, SIB)

    def near_ready(h):
        several(h, 7, 2).wait_recv()

    def pass_far(h):
        arrived(h, 5, to, L)
        go(h, 8, to, L, SIB)
        arrived(h, 6, to, R)
        go(h, 8, to, R, SIB)

    def far_ready(h):
        several(h, 8, 1).wait_recv()

    def up(h, *chips):
        lo, hi = ROWS[0][h]

        def cols_of(cols, width):
            lhs = [xb[pl.ds(2 * b, 2), lo:hi].reshape(128, 2048) for b in chips]
            lhs = lhs[0] if len(lhs) == 1 else jnp.concatenate(lhs, axis=0)
            w = wu[:, :, cols].reshape(2048, width)
            out = jnp.dot(lhs, w, preferred_element_type=F32).astype(BF16)
            for i, b in enumerate(chips):
                for d in range(2):
                    at_row = pl.multiple_of(16 + (2 * b + d) * 128 + lo, 16)
                    ub[pl.ds(at_row, 64), cols] = out[(2 * i + d) * 64 : (2 * i + d + 1) * 64]

        def tile(n, carry):
            cols_of(pl.ds(pl.multiple_of(n * 256, 256), 256), 256)
            return carry

        lax.fori_loop(0, 5, tile, 0)
        cols_of(slice(1280, 1408), 128)

    def halo_copy():
        nxt = lax.rem(me + 1, NSP)
        dev = {"z": lax.div(nxt, 4), "y": lax.rem(nxt, 4)}
        return remote(ub.at[1024:1040, :], halo, h_s.at[0], h_r.at[0], dev)

    def send_halo(when):
        @pl.when(jnp.logical_and(when, me < NSP - 1))
        def _():
            halo_copy().start()

    @pl.when(me == 0)
    def _():
        ub[0:16, :] = jnp.zeros((16, 1408), BF16)

    def conv(g, b):
        lo, hi = ROWS[1][g]
        n_rows = hi - lo
        act = (act0, act1)[g]

        def three(block, half, lanes):
            v = shift_ref[half : half + 1, lanes] + block[14 : 14 + n_rows] * taps_ref[0, half : half + 1, lanes]
            v = v + block[15 : 15 + n_rows] * taps_ref[1, half : half + 1, lanes]
            return v + block[16 : 16 + n_rows] * taps_ref[2, half : half + 1, lanes]

        def device(d, carry):
            around = pl.ds(pl.multiple_of((2 * b + d) * 128 + lo, 16), n_rows + 16)
            rows = pl.ds(pl.multiple_of(d * n_rows, 16), n_rows)
            for n in range(6):
                if n < 5:
                    lanes = slice(n * 128, (n + 1) * 128)
                    gate = ub[around, lanes].astype(F32)
                    value = ub[around, 640 + n * 128 : 640 + (n + 1) * 128].astype(F32)
                else:
                    lanes = slice(640, FF)
                    both = ub[around, 1280:1408].astype(F32)
                    gate, value = both[:, 0:64], pltpu.roll(both, 64, 1)[:, 0:64]
                a = jax.nn.gelu(three(gate, 0, lanes)) * three(value, 1, lanes)
                act[b, rows, lanes] = a.astype(BF16)
            return carry

        lax.fori_loop(0, 2, device, 0)

    def down(g, j, b):
        lo, hi = ROWS[1][g]
        act = (act0, act1)[g]

        def tile(n, carry):
            cols = pl.ds(pl.multiple_of(n * 512, 512), 512)
            p = jnp.dot(act[b], wd[:, cols], preferred_element_type=F32)
            part[1, j, :, lo:hi, cols] = p.astype(BF16).reshape(2, hi - lo, 512)
            return carry

        lax.fori_loop(0, 4, tile, 0)

    B = [Scatter(1, 0), Scatter(1, 1)]
    A[0].finish()
    A[0].each(first_norm)
    own_rows(0)
    A[1].finish()
    A[1].each(first_norm)
    u4()
    n1()
    loaded("taps", "shift")
    arrived(0, 0, t + 1 - 2 * c, W)
    up(0, x)
    send_halo(x == 3)
    pass_on(0)
    own_rows(1)
    pass_second(0)
    arrived(1, 0, t + 1 - 2 * c, W)
    up(1, x)
    n2()
    n3(0)
    n3(1)
    n3(2)
    near_ready(0)
    up(0, xr, xl)
    send_halo(jnp.logical_or(xr == 3, xl == 3))
    pass_far(0)
    conv(0, x)
    conv(0, xr)
    conv(0, xl)
    pass_on(1)
    n3(3)
    far_ready(0)
    up(0, xo)
    send_halo(xo == 3)
    conv(0, xo)
    n4()
    down(0, 0, xo)
    B[0].pair(0).start()
    pass_second(1)
    down(0, 1, xr)
    B[0].pair(1).start()
    B[0].far()
    down(0, 2, xl)
    B[0].pair(2).start()
    B[0].soon_right()
    pass_far(1)
    near_ready(1)
    up(1, xr, xl)
    B[0].soon_left()
    B[0].late()
    far_ready(1)
    up(1, xo)

    @pl.when(me > 0)
    def _():
        halo_copy().wait_recv()
        ub[0:16, :] = halo[...]

    conv(1, xo)
    down(1, 0, xo)
    B[1].pair(0).start()
    conv(1, xr)
    down(1, 1, xr)
    B[1].pair(1).start()
    B[1].far()
    conv(1, xl)
    down(1, 2, xl)
    B[1].pair(2).start()
    B[1].soon_right()
    conv(1, x)
    down(1, 3, x)
    B[1].pair(3).start()
    B[1].soon_left()
    B[1].late()
    down(0, 3, x)
    B[0].pair(3).start()

    def last_norm(r):
        v = ALPHA * xb[t, r, :].astype(F32) + summed(1, r)
        ov[r, :] = normed(v, 1).astype(BF16)

    outs = []
    for g in range(2):
        B[g].finish()
        B[g].each(last_norm)
        lo, hi = ROWS[1][g]
        outs.append(pltpu.make_async_copy(ov.at[lo:hi], o_ref.at[lo:hi], out_sem.at[g]))
        outs[g].start()

    scattered.wait_send()
    returned.wait_send()
    udrain()
    ndrain()
    for op in A + B:
        op.drain()
    for h in range(2):
        several(h, 0, 7).wait_send()

    @pl.when(me < NSP - 1)
    def _():
        halo_copy().wait_send()

    for op in outs:
        op.wait()


def shards(q, k, v, g, logd, res, ow, gain, bias, ug, uv, cw, cbias, dw):
    ti, tb = position_tables()
    dma = pltpu.SemaphoreType.DMA
    hb = pl.BlockSpec(memory_space=pl.ANY)
    return pl.pallas_call(
        body,
        out_shape=jax.ShapeDtypeStruct((128, 2048), BF16),
        in_specs=[hb] * 16,
        out_specs=hb,
        scratch_shapes=[
            pltpu.VMEM((1024, 256), BF16),
            pltpu.VMEM((1024, 256), BF16),
            pltpu.VMEM((1024, 512), BF16),
            pltpu.VMEM((1024, 512), BF16),
            pltpu.VMEM((8, 128), F32),
            pltpu.VMEM((128, 2048), BF16),
            pltpu.VMEM((512, 2048), BF16),
            pltpu.VMEM((2, 2048), F32),
            pltpu.VMEM((2, 2048), F32),
            pltpu.VMEM((1408, 128), BF16),
            pltpu.VMEM((3, 2, FF), F32),
            pltpu.VMEM((2, FF), F32),
            pltpu.VMEM((2, BLK, 128), F32),
            pltpu.VMEM((8, 128), F32),
            pltpu.VMEM((NSP, 128, 1408), BF16),
            pltpu.VMEM((FFP, 2048), BF16),
            pltpu.VMEM((8, 256), F32),
            pltpu.VMEM((8, 256), F32),
            pltpu.VMEM((256, 8), F32),
            pltpu.VMEM((4, 8, 128), F32),
            pltpu.VMEM((4, 256, 256), BF16),
            pltpu.VMEM((4, 256, 256), BF16),
            pltpu.VMEM((5, 256, 512), F32),
            pltpu.VMEM((4, 256, 512), F32),
            pltpu.VMEM((256, 512), BF16),
            pltpu.VMEM((NSP, 16, 640), BF16),
            pltpu.VMEM((NSP, 16, 640), BF16),
            pltpu.VMEM((NSP, 16, 512), BF16),
            pltpu.VMEM((NSP, 16, 512), BF16),
            pltpu.VMEM((2, 4, 2, 128, 2048), BF16),
            pltpu.VMEM((2, 4, 128, 2048), BF16),
            pltpu.VMEM((2, 3, 128, 2048), BF16),
            pltpu.VMEM((2, 128, 1024), BF16),
            pltpu.VMEM((2, 128, 1024), BF16),
            pltpu.VMEM((2, 128, 2048), BF16),
            pltpu.VMEM((2, 128, 2048), BF16),
            pltpu.VMEM((8, 128, 2048), BF16),
            pltpu.VMEM((1040, 1408), BF16),
            pltpu.VMEM((4, 96, FFP), BF16),
            pltpu.VMEM((4, 160, FFP), BF16),
            pltpu.VMEM((16, 1408), BF16),
            pltpu.VMEM((128, 2048), BF16),
            dma((18,)),
            dma((2,)),
            dma((2,)),
            dma((2,)),
            dma((2, 7)),
            dma((2, 2)),
            dma((2, 2, 4)),
            dma((2, 2)),
            dma((2, 2, 3)),
            dma((2,)),
            dma((2, 9)),
            dma((1,)),
            dma((1,)),
            dma((2,)),
        ],
        compiler_params=pltpu.CompilerParams(
            collective_id=0, has_side_effects=True, vmem_limit_bytes=62 * 1024 * 1024
        ),
        name="layer",
    )(
        q, k, v, g, logd.reshape(8, 128), res, ow, gain, bias, ug.T, uv.T,
        cw.transpose(1, 0, 2), cbias, dw, ti, tb,
    )


def solution(mesh):
    torus = Mesh(mesh.devices.reshape(4, 4, 4, 2), ("z", "y", "x", "c"))
    sp, tp = ("z", "y"), ("x", "c")
    return jax.shard_map(
        shards,
        mesh=torus,
        in_specs=(
            P(sp, tp),
            P(sp, tp),
            P(sp, tp),
            P(sp, tp),
            P(sp, tp),
            P(sp, None),
            P(tp, None),
            P(),
            P(),
            P(sp, tp),
            P(sp, tp),
            P(None, None, tp),
            P(None, tp),
            P(tp, sp),
        ),
        out_specs=P(sp + tp, None),
        check_vma=False,
    )
```

```python
import functools

import jax
import jax.numpy as jnp
import numpy as np
from jax import lax
from jax.experimental import pallas as pl
from jax.experimental.pallas import tpu as pltpu
from jax.sharding import Mesh
from jax.sharding import PartitionSpec as P

F32 = jnp.float32
BF16 = jnp.bfloat16
HIGH = lax.Precision.HIGHEST
MESH = pl.DeviceIdType.MESH
ALPHA = 8.0**0.25
EPS = 1e-05
NSP = 16
BLK = 256
FF = 704
FFP = 768
ROWS = (((48, 128), (0, 48)), ((64, 128), (0, 64)))
NT = (((1,), (1,)), ((), ()))
TN = (((0,), (0,)), ((), ()))


def position_tables():
    freq = 10000.0 ** (-2.0 * np.arange(128, dtype=np.float64) / 256.0)
    inner = np.arange(BLK, dtype=np.float64)[:, None] * freq[None]
    start = np.arange(4 * NSP, dtype=np.float64)[:, None] * BLK * freq[None]
    ti = np.stack([np.cos(inner), np.sin(inner)]).astype(np.float32)
    tb = np.concatenate(
        [np.cos(start).reshape(NSP, 4, 128), np.sin(start).reshape(NSP, 4, 128)], axis=1
    ).astype(np.float32)
    return ti, tb


def body(
    q_h, k_h, v_h, g_h, log_h, res_h, ow_h, gain_h, bias_h, ug_h, uv_h, taps_h, shift_h, dw_h,
    ti_h, tb_h, o_ref,
    qv, kv, vv, gv, log_ref, rv, owv, gain_ref, bias_ref, ust, taps_ref, shift_ref, ti_ref, tb_ref,
    wu, wd,
    lsc, crow, ccol, dpre, kr, sq, loc, within, gr,
    ssend, srecv, rsend, inc,
    part, d2, cb, ra, rb, rl, rr,
    xb, ub, act0, act1, halo, ov,
    in_sem, st_s, st_r, wg_s, wg_r, d2_s, d2_r, x_s, x_r, ag_s, ag_r, h_s, h_r, out_sem,
):
    z, y, x, c = (lax.axis_index(a) for a in ("z", "y", "x", "c"))
    me = z * 4 + y
    t = x * 2 + c
    xr, xl, xo = lax.rem(x + 1, 4), lax.rem(x + 3, 4), lax.rem(x + 2, 4)

    def at(axis, value):
        return {axis: value}

    SIB = at("c", 1 - c)
    XR, XL = at("x", xr), at("x", xl)

    def remote(src, dst, ssem, rsem, dev):
        return pltpu.make_async_remote_copy(
            src_ref=src, dst_ref=dst, send_sem=ssem, recv_sem=rsem, device_id=dev,
            device_id_type=MESH,
        )

    loads = {
        "log": (log_h, log_ref),
        "k": (k_h, kv),
        "ti": (ti_h, ti_ref),
        "tb": (tb_h.at[me], tb_ref),
        "v": (v_h, vv),
        "ug": (ug_h.at[0:640], ust.at[0:640]),
        "uv": (uv_h.at[0:640], ust.at[640:1280]),
        "ug2": (ug_h.at[640:704], ust.at[1280:1344]),
        "uv2": (uv_h.at[640:704], ust.at[1344:1408]),
        "q": (q_h, qv),
        "g": (g_h, gv),
        "ow": (ow_h, owv),
        "dw": (dw_h, wd.at[0:FF, pl.ds(pl.multiple_of(me * 128, 128), 128)]),
        "res": (res_h.at[pl.ds(pl.multiple_of(t * 128, 128), 128)], rv),
        "gain": (gain_h, gain_ref),
        "bias": (bias_h, bias_ref),
        "taps": (taps_h, taps_ref),
        "shift": (shift_h, shift_ref),
    }
    loads = {
        name: pltpu.make_async_copy(src, dst, in_sem.at[5 if i in (6, 7, 8) else i])
        for i, (name, (src, dst)) in enumerate(loads.items())
    }
    for load in loads.values():
        load.start()

    def loaded(*names):
        for name in names:
            loads[name].wait()

    barrier = pltpu.get_barrier_semaphore()

    def sp_peer(i):
        j = lax.rem(me + i, NSP)
        return j, {"z": lax.div(j, 4), "y": lax.rem(j, 4)}

    def greet(i, carry):
        _, dev = sp_peer(i)
        pl.semaphore_signal(barrier, inc=1, device_id=dev, device_id_type=MESH)
        return carry

    lax.fori_loop(1, NSP, greet, 0)
    for dev in (SIB, XR, XL):
        pl.semaphore_signal(barrier, inc=1, device_id=dev, device_id_type=MESH)

    yr, yl, yo = lax.rem(y + 1, 4), lax.rem(y + 3, 4), lax.rem(y + 2, 4)
    zr, zl, zo = lax.rem(z + 1, 4), lax.rem(z + 3, 4), lax.rem(z + 2, 4)
    YR, YL, ZR, ZL = at("y", yr), at("y", yl), at("z", zr), at("z", zl)

    def up_piece(zz, yy, lo, n):
        return wu.at[zz * 4 + yy, lo * 16 : (lo + n) * 16, :]

    def dn_piece(zz, yy, lo, n):
        col = pl.multiple_of((zz * 4 + yy) * 128, 128)
        return wd.at[lo * 88 : (lo + n) * 88, pl.ds(col, 128)]

    def gather(g, piece, bytes_of):
        def put(n, zz, yy, lo, cnt, dev):
            p = piece(zz, yy, lo, cnt)
            remote(p, p, wg_s.at[g], wg_r.at[g, n], dev).start()

        def got(n, shards):
            p = bytes_of(shards)
            remote(p, p, wg_s.at[g], wg_r.at[g, n], YR).wait_recv()

        def s0():
            put(0, z, y, 0, 4, YR)
            put(0, z, y, 0, 4, YL)
            put(0, z, y, 4, 4, ZR)
            put(0, z, y, 4, 4, ZL)

        def s0b():
            put(2, z, y, 0, 4, ZR)
            put(2, z, y, 0, 4, ZL)
            put(2, z, y, 4, 4, YR)
            put(2, z, y, 4, 4, YL)

        def s1():
            got(0, 2)
            put(1, z, yl, 0, 2, YR)
            put(1, z, yr, 2, 2, YL)
            put(1, zl, y, 4, 2, ZR)
            put(1, zr, y, 6, 2, ZL)
            put(3, z, yl, 0, 4, ZR)
            put(3, z, yl, 0, 4, ZL)
            put(3, zl, y, 4, 4, YR)
            put(3, zl, y, 4, 4, YL)
            put(4, z, yr, 0, 4, ZR)
            put(4, z, yr, 0, 4, ZL)
            put(4, zr, y, 4, 4, YR)
            put(4, zr, y, 4, 4, YL)

        def s2():
            got(1, 1)
            put(5, z, yo, 0, 4, ZR)
            put(5, z, yo, 0, 4, ZL)
            put(5, zo, y, 4, 4, YR)
            put(5, zo, y, 4, 4, YL)

        def s3(m):
            ym, zm = (y, yl, yr, yo)[m], (z, zl, zr, zo)[m]
            got(2 + m, 2)
            put(6, zl, ym, 0, 2, ZR)
            put(6, zr, ym, 2, 2, ZL)
            put(6, zm, yl, 4, 2, YR)
            put(6, zm, yr, 6, 2, YL)

        def s4():
            got(6, 4)

        def drain():
            p = bytes_of(15)
            remote(p, p, wg_s.at[g], wg_r.at[g, 0], YR).wait_send()

        return s0, s0b, s1, s2, s3, s4, drain

    u0, u0b, u1, u2, u3, u4, udrain = gather(0, up_piece, lambda n: wu.at[0:n])
    n0, n0b, n1, n2, n3, n4, ndrain = gather(1, dn_piece, lambda n: wd.at[0:FF, 0 : n * 128])

    ri = lax.broadcasted_iota(jnp.int32, (BLK, BLK), 0)
    ci = lax.broadcasted_iota(jnp.int32, (BLK, BLK), 1)
    causal = ri >= ci
    tri = jnp.where(causal, 1.0, 0.0).astype(F32)
    lsc[...] = jnp.zeros((8, 256), F32)
    loaded("log")
    for b in range(4):
        lsc[b : b + 1, 0:128] = log_ref[2 * b : 2 * b + 1, :]
        lsc[b : b + 1, 128:256] = log_ref[2 * b + 1 : 2 * b + 2, :]
    logs = lsc[...]
    crow[...] = lax.dot_general(logs, tri, NT, precision=HIGH, preferred_element_type=F32)
    ccol[...] = lax.dot_general(tri, logs, NT, precision=HIGH, preferred_element_type=F32)
    loaded("k", "ti", "tb", "v")
    base = tb_ref[...]

    def turned(ref, b):
        ci_, si_ = ti_ref[0], ti_ref[1]
        cb_, sb_ = base[b : b + 1, :], base[4 + b : 5 + b, :]
        cos = cb_ * ci_ - sb_ * si_
        sin = sb_ * ci_ + cb_ * si_
        front = ref[b * BLK : (b + 1) * BLK, 0:128].astype(F32)
        second = ref[b * BLK : (b + 1) * BLK, 128:256].astype(F32)
        return front * cos - second * sin, front * sin + second * cos

    decay = jnp.ones((1, 1), F32)
    for b in range(4):
        front, second = turned(kv, b)
        front = (front * 0.0625).astype(BF16)
        second = (second * 0.0625).astype(BF16)
        kr[b, :, 0:128] = front
        kr[b, :, 128:256] = second
        total = crow[b : b + 1, 255:256]
        to_end = jnp.exp(total - ccol[:, b : b + 1])
        faded = jnp.concatenate([front, second], axis=1).astype(F32) * to_end
        state = lax.dot_general(
            faded.astype(BF16), vv[b * BLK : (b + 1) * BLK, :], TN, preferred_element_type=F32
        )
        step = jnp.exp(total)
        dpre[b] = jnp.broadcast_to(decay, (8, 128))
        decay = decay * step
        if b == 0:
            loc[b] = jnp.zeros((BLK, 512), F32)
            loc[b + 1] = state
        else:
            loc[b + 1] = step * loc[b] + state

    hi = decay.astype(BF16)
    mid = (decay - hi.astype(F32)).astype(BF16)
    low = (decay - hi.astype(F32) - mid.astype(F32)).astype(BF16)
    row = lax.broadcasted_iota(jnp.int32, (16, 128), 0)
    tag = jnp.where(
        row == 0,
        hi.astype(F32),
        jnp.where(row == 1, mid.astype(F32), jnp.where(row == 2, low.astype(F32), 0.0)),
    ).astype(BF16)
    for j in range(NSP):
        ssend[j, :, 0:512] = loc[4, j * 16 : (j + 1) * 16, :].astype(BF16)
        ssend[j, :, 512:640] = tag

    pl.semaphore_wait(barrier, NSP + 2)

    def scatter(i, carry):
        j, dev = sp_peer(i)
        remote(ssend.at[j], srecv.at[me], st_s.at[0], st_r.at[0], dev).start()
        return carry

    lax.fori_loop(1, NSP, scatter, 0)
    srecv[me] = ssend[me]

    pltpu.make_async_copy(ust, ust, in_sem.at[5]).wait()
    for n in range(11):
        tile = ust[n * 128 : (n + 1) * 128, :].astype(F32)
        wu[me, :, n * 128 : (n + 1) * 128] = tile.T.astype(BF16)
    u0()

    loaded("q")
    for b in range(4):
        front, second = turned(qv, b)
        qr = jnp.concatenate([front, second], axis=1).astype(BF16)
        column = ccol[:, b : b + 1]
        sq[b] = (qr.astype(F32) * jnp.exp(column)).astype(BF16)
        scores = lax.dot_general(qr, kr[b], NT, preferred_element_type=F32)
        gap = column - crow[b : b + 1, :]
        weight = jnp.where(causal, jnp.exp(jnp.where(causal, gap, 0.0)), 0.0)
        within[b] = jnp.dot(
            (scores * weight).astype(BF16),
            vv[b * BLK : (b + 1) * BLK, :],
            preferred_element_type=F32,
        )
    wd[FF:FFP, :] = jnp.zeros((FFP - FF, 2048), BF16)
    act0[:, :, FF:FFP] = jnp.zeros((4, 128, FFP - FF), BF16)
    act1[:, :, FF:FFP] = jnp.zeros((4, 128, FFP - FF), BF16)

    fifteen = slice(0, NSP - 1)
    scattered = remote(ssend.at[fifteen], srecv.at[fifteen], st_s.at[0], st_r.at[0], YR)
    returned = remote(rsend.at[fifteen], inc.at[fifteen], st_s.at[1], st_r.at[1], YR)
    scattered.wait_recv()
    acc = jnp.zeros((16, 512), F32)
    for d in range(NSP):
        rsend[d] = acc.astype(BF16)
        if d < NSP - 1:
            tags = srecv[d, :, 512:640].astype(F32)
            factor = tags[0:1, 0:1] + tags[1:2, 0:1] + tags[2:3, 0:1]
            acc = factor * acc + srecv[d, :, 0:512].astype(F32)
    inc[me] = rsend[me]

    def give_back(i, carry):
        j, dev = sp_peer(i)
        remote(rsend.at[j], inc.at[me], st_s.at[1], st_r.at[1], dev).start()
        return carry

    lax.fori_loop(1, NSP, give_back, 0)
    u0b()
    u1()

    returned.wait_recv()

    order = (xo, xr, xl, x)
    L, R = slice(0, 1024), slice(1024, 2048)

    class Scatter:
        def __init__(self, s, h):
            self.s, self.h = s, h
            self.lo, self.hi = ROWS[s][h]
            rows = slice(self.lo, self.hi)

            def across(n, src, dst, dev):
                return remote(src, dst, x_s.at[s, h], x_r.at[s, h, n], dev)

            self.a_out = across(0, cb.at[s, 0, rows, L], ra.at[s, rows], XR)
            self.b_out = across(1, cb.at[s, 0, rows, R], rb.at[s, rows], XL)
            self.r_late = across(2, cb.at[s, 1, rows, L], rl.at[s, rows, L], XR)
            self.r_soon = across(2, cb.at[s, 1, rows, R], rl.at[s, rows, R], XR)
            self.l_soon = across(2, cb.at[s, 2, rows, L], rr.at[s, rows, L], XL)
            self.l_late = across(2, cb.at[s, 2, rows, R], rr.at[s, rows, R], XL)
            self.into = across(2, cb.at[s, 0:2, rows], d2.at[s, 0:2, rows], XR)
            self.away = across(2, cb.at[s, 0:3, rows], d2.at[s, 0:3, rows], XR)

        def pair(self, j):
            s, h, rows = self.s, self.h, slice(self.lo, self.hi)
            return remote(
                part.at[s, j, 1 - c, rows], d2.at[s, j, rows], d2_s.at[s, h], d2_r.at[s, h, j], SIB
            )

        def merged(self, j, cols, extra=None):
            s = self.s

            for r in self.steps():
                v = part[s, j, c, r, cols].astype(F32) + d2[s, j, r, cols].astype(F32)
                if extra is not None:
                    v = v + extra[s, r, :].astype(F32)
                cb[s, j, r, cols] = v.astype(BF16)

        def steps(self):
            return [slice(r, min(r + 32, self.hi)) for r in range(self.lo, self.hi, 32)]

        def far(self):
            self.pair(0).wait_recv()
            self.merged(0, L)
            self.a_out.start()
            self.merged(0, R)
            self.b_out.start()

        def soon_right(self):
            self.pair(1).wait_recv()
            self.merged(1, R)
            self.r_soon.start()

        def soon_left(self):
            self.pair(2).wait_recv()
            self.merged(2, L)
            self.l_soon.start()

        def late(self):
            self.a_out.wait_recv()
            self.merged(1, L, ra)
            self.r_late.start()
            self.b_out.wait_recv()
            self.merged(2, R, rb)
            self.l_late.start()

        def finish(self):
            self.pair(3).wait_recv()
            self.into.wait_recv()

        def each(self, step):
            for r in self.steps():
                step(r)

        def drain(self):
            s, h, rows = self.s, self.h, slice(self.lo, self.hi)
            remote(
                d2.at[s, :, rows], d2.at[s, :, rows], d2_s.at[s, h], d2_r.at[s, h, 0], SIB
            ).wait_send()
            self.away.wait_send()

    def summed(s, r):
        v = part[s, 3, c, r, :].astype(F32) + d2[s, 3, r, :].astype(F32)
        return v + rl[s, r, :].astype(F32) + rr[s, r, :].astype(F32)

    def normed(v, i):
        mean = jnp.mean(v, axis=-1, keepdims=True)
        v = v - mean
        var = jnp.mean(v * v, axis=-1, keepdims=True)
        return v * lax.rsqrt(var + EPS) * gain_ref[i : i + 1, :] + bias_ref[i : i + 1, :]

    loaded("g", "ow")

    def mix(b):
        rows = pl.ds(pl.multiple_of(b * BLK, BLK), BLK)
        state = dpre[b][0:1, 0:1] * inc[...].reshape(BLK, 512).astype(F32) + loc[b]
        mixed = within[b] + jnp.dot(sq[b], state.astype(BF16), preferred_element_type=F32)
        mean = jnp.mean(mixed, axis=-1, keepdims=True)
        mixed = mixed - mean
        var = jnp.mean(mixed * mixed, axis=-1, keepdims=True)
        mixed = mixed * lax.rsqrt(var + EPS)
        gate = gv[rows, :].astype(F32)
        gr[...] = (gate * jax.nn.sigmoid(gate) * mixed).astype(BF16).reshape(2, 128, 512)

    def project(j, lo=0, hi=128):
        def tile(n, carry):
            cols = pl.ds(pl.multiple_of(n * 512, 512), 512)
            lhs = gr[:, lo:hi].reshape(2 * (hi - lo), 512)
            p = jnp.dot(lhs, owv[:, cols], preferred_element_type=F32)
            part[0, j, :, lo:hi, cols] = p.astype(BF16).reshape(2, hi - lo, 512)
            return carry

        lax.fori_loop(0, 4, tile, 0)

    A = [Scatter(0, 0), Scatter(0, 1)]
    mix(order[0])
    for h in A:
        project(0, h.lo, h.hi)
        h.pair(0).start()
    mix(order[1])
    A[0].far()
    project(1)
    for h in A:
        h.pair(1).start()
    mix(order[2])
    project(2)
    for h in A:
        h.pair(2).start()
    A[0].soon_right()
    A[1].far()
    mix(order[3])
    project(3)
    for h in A:
        h.pair(3).start()
    A[0].soon_left()
    A[0].late()
    A[1].soon_right()
    A[1].soon_left()
    u2()
    u3(0)
    u3(1)
    u3(2)
    A[1].late()
    u3(3)
    loaded("dw")
    n0()
    n0b()
    loaded("res", "gain", "bias")

    def first_norm(r):
        v = ALPHA * rv[r, :].astype(F32) + summed(0, r)
        xb[t, r, :] = normed(v, 0).astype(BF16)

    tl, tr, to = xl * 2 + c, xr * 2 + c, xo * 2 + c
    W = slice(0, 2048)

    def ag(h, n, owner, cols, dev):
        lo, hi = ROWS[0][h]
        p = xb.at[owner, lo:hi, cols]
        return remote(p, p, ag_s.at[h], ag_r.at[h, n], dev)

    def go(h, n, owner, cols, dev):
        ag(h, n, owner, cols, dev).start()

    def several(h, n, owners):
        lo, hi = ROWS[0][h]
        p = xb.at[0:owners, lo:hi]
        return remote(p, p, ag_s.at[h], ag_r.at[h, n], SIB)

    def arrived(h, n, owner, cols):
        ag(h, n, owner, cols, SIB).wait_recv()

    def own_rows(h):
        go(h, 1, t, L, XR)
        go(h, 3, t, R, XL)
        if h == 0:
            go(h, 0, t, W, SIB)
        go(h, 2, t, R, XR)
        go(h, 4, t, L, XL)

    def pass_on(h):
        arrived(h, 1, tl, L)
        go(h, 5, tl, L, XR)
        arrived(h, 3, tr, R)
        go(h, 6, tr, R, XL)
        go(h, 7, tl, L, SIB)
        go(h, 7, tr, R, SIB)

    def pass_second(h):
        arrived(h, 2, tl, R)
        go(h, 7, tl, R, SIB)
        arrived(h, 4, tr, L)
        go(h, 7, tr, L, SIB)

    def near_ready(h):
        several(h, 7, 2).wait_recv()

    def pass_far(h):
        arrived(h, 5, to, L)
        go(h, 8, to, L, SIB)
        arrived(h, 6, to, R)
        go(h, 8, to, R, SIB)

    def far_ready(h):
        several(h, 8, 1).wait_recv()

    def up(h, *chips):
        lo, hi = ROWS[0][h]
        rows = hi - lo

        def cols_of(cols, width):
            lhs = [xb[pl.ds(2 * b, 2), lo:hi].reshape(2 * rows, 2048) for b in chips]
            lhs = lhs[0] if len(lhs) == 1 else jnp.concatenate(lhs, axis=0)
            w = wu[:, :, cols].reshape(2048, width)
            out = jnp.dot(lhs, w, preferred_element_type=F32).astype(BF16)
            for i, b in enumerate(chips):
                for d in range(2):
                    at_row = pl.multiple_of(16 + (2 * b + d) * 128 + lo, 16)
                    ub[pl.ds(at_row, rows), cols] = out[(2 * i + d) * rows : (2 * i + d + 1) * rows]

        def tile(n, carry):
            cols_of(pl.ds(pl.multiple_of(n * 256, 256), 256), 256)
            return carry

        lax.fori_loop(0, 5, tile, 0)
        cols_of(slice(1280, 1408), 128)

    def halo_copy():
        nxt = lax.rem(me + 1, NSP)
        dev = {"z": lax.div(nxt, 4), "y": lax.rem(nxt, 4)}
        return remote(ub.at[1024:1040, :], halo, h_s.at[0], h_r.at[0], dev)

    def send_halo(when):
        @pl.when(jnp.logical_and(when, me < NSP - 1))
        def _():
            halo_copy().start()

    @pl.when(me == 0)
    def _():
        ub[0:16, :] = jnp.zeros((16, 1408), BF16)

    def conv(g, b):
        lo, hi = ROWS[1][g]
        n_rows = hi - lo
        act = (act0, act1)[g]

        def three(block, half, lanes):
            v = shift_ref[half : half + 1, lanes] + block[14 : 14 + n_rows] * taps_ref[0, half : half + 1, lanes]
            v = v + block[15 : 15 + n_rows] * taps_ref[1, half : half + 1, lanes]
            return v + block[16 : 16 + n_rows] * taps_ref[2, half : half + 1, lanes]

        def device(d, carry):
            around = pl.ds(pl.multiple_of((2 * b + d) * 128 + lo, 16), n_rows + 16)
            rows = pl.ds(pl.multiple_of(d * n_rows, 16), n_rows)
            for n in range(6):
                if n < 5:
                    lanes = slice(n * 128, (n + 1) * 128)
                    gate = ub[around, lanes].astype(F32)
                    value = ub[around, 640 + n * 128 : 640 + (n + 1) * 128].astype(F32)
                else:
                    lanes = slice(640, FF)
                    both = ub[around, 1280:1408].astype(F32)
                    gate, value = both[:, 0:64], pltpu.roll(both, 64, 1)[:, 0:64]
                a = jax.nn.gelu(three(gate, 0, lanes)) * three(value, 1, lanes)
                act[b, rows, lanes] = a.astype(BF16)
            return carry

        lax.fori_loop(0, 2, device, 0)

    def down(g, js, chips):
        lo, hi = ROWS[1][g]
        act = (act0, act1)[g]

        def tile(n, carry):
            cols = pl.ds(pl.multiple_of(n * 512, 512), 512)
            lhs = [act[b] for b in chips]
            lhs = lhs[0] if len(lhs) == 1 else jnp.concatenate(lhs, axis=0)
            p = jnp.dot(lhs, wd[:, cols], preferred_element_type=F32).astype(BF16)
            p = p.reshape(len(js), 2, hi - lo, 512)
            for i, j in enumerate(js):
                part[1, j, :, lo:hi, cols] = p[i]
            return carry

        lax.fori_loop(0, 4, tile, 0)

    B = [Scatter(1, 0), Scatter(1, 1)]
    A[0].finish()
    A[0].each(first_norm)
    own_rows(0)
    A[1].finish()
    A[1].each(first_norm)
    go(1, 0, t, W, SIB)
    u4()
    loaded("taps", "shift")
    arrived(0, 0, t + 1 - 2 * c, W)
    up(0, x)
    send_halo(x == 3)
    pass_on(0)
    own_rows(1)
    n1()
    conv(0, x)
    pass_second(0)
    arrived(1, 0, t + 1 - 2 * c, W)
    up(1, x)
    near_ready(0)
    n2()
    n3(0)
    up(0, xr, xl)
    send_halo(jnp.logical_or(xr == 3, xl == 3))
    pass_far(0)
    n3(1)
    conv(0, xr)
    conv(0, xl)
    pass_on(1)
    n3(2)
    n3(3)
    far_ready(0)
    up(0, xo)
    send_halo(xo == 3)
    pass_second(1)
    conv(0, xo)
    n4()
    down(0, (0,), (xo,))
    B[0].pair(0).start()
    down(0, (1, 2), (xr, xl))
    B[0].pair(1).start()
    B[0].pair(2).start()
    pass_far(1)
    B[0].far()
    down(0, (3,), (x,))
    B[0].pair(3).start()
    B[0].soon_right()
    B[0].soon_left()
    near_ready(1)
    far_ready(1)
    up(1, xo, xr, xl)

    @pl.when(me > 0)
    def _():
        halo_copy().wait_recv()
        ub[0:16, :] = halo[...]

    conv(1, xo)
    down(1, (0,), (xo,))
    B[1].pair(0).start()
    B[0].late()
    conv(1, xr)
    down(1, (1,), (xr,))
    B[1].pair(1).start()
    B[1].far()
    conv(1, xl)
    down(1, (2,), (xl,))
    B[1].pair(2).start()
    B[1].soon_right()
    conv(1, x)
    down(1, (3,), (x,))
    B[1].pair(3).start()
    B[1].soon_left()

    def last_norm(r):
        v = ALPHA * xb[t, r, :].astype(F32) + summed(1, r)
        ov[r, :] = normed(v, 1).astype(BF16)

    outs = []
    for g in range(2):
        if g == 1:
            B[g].late()
        B[g].finish()
        B[g].each(last_norm)
        lo, hi = ROWS[1][g]
        outs.append(pltpu.make_async_copy(ov.at[lo:hi], o_ref.at[lo:hi], out_sem.at[g]))
        outs[g].start()

    scattered.wait_send()
    returned.wait_send()
    udrain()
    ndrain()
    for op in A + B:
        op.drain()
    for h in range(2):
        several(h, 0, 7).wait_send()

    @pl.when(me < NSP - 1)
    def _():
        halo_copy().wait_send()

    for op in outs:
        op.wait()


def shards(q, k, v, g, logd, res, ow, gain, bias, ug, uv, cw, cbias, dw):
    ti, tb = position_tables()
    dma = pltpu.SemaphoreType.DMA
    hb = pl.BlockSpec(memory_space=pl.ANY)
    return pl.pallas_call(
        body,
        out_shape=jax.ShapeDtypeStruct((128, 2048), BF16),
        in_specs=[hb] * 16,
        out_specs=hb,
        scratch_shapes=[
            pltpu.VMEM((1024, 256), BF16),
            pltpu.VMEM((1024, 256), BF16),
            pltpu.VMEM((1024, 512), BF16),
            pltpu.VMEM((1024, 512), BF16),
            pltpu.VMEM((8, 128), F32),
            pltpu.VMEM((128, 2048), BF16),
            pltpu.VMEM((512, 2048), BF16),
            pltpu.VMEM((2, 2048), F32),
            pltpu.VMEM((2, 2048), F32),
            pltpu.VMEM((1408, 128), BF16),
            pltpu.VMEM((3, 2, FF), F32),
            pltpu.VMEM((2, FF), F32),
            pltpu.VMEM((2, BLK, 128), F32),
            pltpu.VMEM((8, 128), F32),
            pltpu.VMEM((NSP, 128, 1408), BF16),
            pltpu.VMEM((FFP, 2048), BF16),
            pltpu.VMEM((8, 256), F32),
            pltpu.VMEM((8, 256), F32),
            pltpu.VMEM((256, 8), F32),
            pltpu.VMEM((4, 8, 128), F32),
            pltpu.VMEM((4, 256, 256), BF16),
            pltpu.VMEM((4, 256, 256), BF16),
            pltpu.VMEM((5, 256, 512), F32),
            pltpu.VMEM((4, 256, 512), F32),
            pltpu.VMEM((2, 128, 512), BF16),
            pltpu.VMEM((NSP, 16, 640), BF16),
            pltpu.VMEM((NSP, 16, 640), BF16),
            pltpu.VMEM((NSP, 16, 512), BF16),
            pltpu.VMEM((NSP, 16, 512), BF16),
            pltpu.VMEM((2, 4, 2, 128, 2048), BF16),
            pltpu.VMEM((2, 4, 128, 2048), BF16),
            pltpu.VMEM((2, 3, 128, 2048), BF16),
            pltpu.VMEM((2, 128, 1024), BF16),
            pltpu.VMEM((2, 128, 1024), BF16),
            pltpu.VMEM((2, 128, 2048), BF16),
            pltpu.VMEM((2, 128, 2048), BF16),
            pltpu.VMEM((8, 128, 2048), BF16),
            pltpu.VMEM((1040, 1408), BF16),
            pltpu.VMEM((4, 128, FFP), BF16),
            pltpu.VMEM((4, 128, FFP), BF16),
            pltpu.VMEM((16, 1408), BF16),
            pltpu.VMEM((128, 2048), BF16),
            dma((18,)),
            dma((2,)),
            dma((2,)),
            dma((2,)),
            dma((2, 7)),
            dma((2, 2)),
            dma((2, 2, 4)),
            dma((2, 2)),
            dma((2, 2, 3)),
            dma((2,)),
            dma((2, 9)),
            dma((1,)),
            dma((1,)),
            dma((2,)),
        ],
        compiler_params=pltpu.CompilerParams(
            collective_id=0, has_side_effects=True, vmem_limit_bytes=62 * 1024 * 1024
        ),
        name="layer",
    )(
        q, k, v, g, logd.reshape(8, 128), res, ow, gain, bias, ug.T, uv.T,
        cw.transpose(1, 0, 2), cbias, dw, ti, tb,
    )


def solution(mesh):
    torus = Mesh(mesh.devices.reshape(4, 4, 4, 2), ("z", "y", "x", "c"))
    sp, tp = ("z", "y"), ("x", "c")
    return jax.shard_map(
        shards,
        mesh=torus,
        in_specs=(
            P(sp, tp),
            P(sp, tp),
            P(sp, tp),
            P(sp, tp),
            P(sp, tp),
            P(sp, None),
            P(tp, None),
            P(),
            P(),
            P(sp, tp),
            P(sp, tp),
            P(None, None, tp),
            P(None, tp),
            P(tp, sp),
        ),
        out_specs=P(sp + tp, None),
        check_vma=False,
    )
```

```python
import functools

import jax
import jax.numpy as jnp
import numpy as np
from jax import lax
from jax.experimental import pallas as pl
from jax.experimental.pallas import tpu as pltpu
from jax.sharding import Mesh
from jax.sharding import PartitionSpec as P

F32 = jnp.float32
BF16 = jnp.bfloat16
HIGH = lax.Precision.HIGHEST
MESH = pl.DeviceIdType.MESH
ALPHA = 8.0**0.25
EPS = 1e-05
NSP = 16
BLK = 256
FF = 704
FFP = 768
ROWS = (((48, 128), (0, 48)), ((64, 128), (0, 64)))
NT = (((1,), (1,)), ((), ()))
TN = (((0,), (0,)), ((), ()))


def position_tables():
    freq = 10000.0 ** (-2.0 * np.arange(128, dtype=np.float64) / 256.0)
    inner = np.arange(BLK, dtype=np.float64)[:, None] * freq[None]
    start = np.arange(4 * NSP, dtype=np.float64)[:, None] * BLK * freq[None]
    ti = np.stack([np.cos(inner), np.sin(inner)]).astype(np.float32)
    tb = np.concatenate(
        [np.cos(start).reshape(NSP, 4, 128), np.sin(start).reshape(NSP, 4, 128)], axis=1
    ).astype(np.float32)
    return ti, tb


def body(
    q_h, k_h, v_h, g_h, log_h, res_h, ow_h, gain_h, bias_h, ug_h, uv_h, taps_h, shift_h, dw_h,
    ti_h, tb_h, o_ref,
    qv, kv, vv, gv, log_ref, rv, owv, gain_ref, bias_ref, ust, taps_ref, shift_ref, ti_ref, tb_ref,
    wu, wd,
    lsc, crow, ccol, dpre, kr, sq, loc, within, gr,
    ssend, srecv, rsend, inc,
    part, d2, cb, ra, rb, rl, rr,
    xb, ub, act0, act1, halo, ov,
    in_sem, st_s, st_r, wg_s, wg_r, d2_s, d2_r, x_s, x_r, ag_s, ag_r, h_s, h_r, out_sem,
):
    z, y, x, c = (lax.axis_index(a) for a in ("z", "y", "x", "c"))
    me = z * 4 + y
    t = x * 2 + c
    xr, xl, xo = lax.rem(x + 1, 4), lax.rem(x + 3, 4), lax.rem(x + 2, 4)

    def at(axis, value):
        return {axis: value}

    SIB = at("c", 1 - c)
    XR, XL = at("x", xr), at("x", xl)

    def remote(src, dst, ssem, rsem, dev):
        return pltpu.make_async_remote_copy(
            src_ref=src, dst_ref=dst, send_sem=ssem, recv_sem=rsem, device_id=dev,
            device_id_type=MESH,
        )

    loads = {
        "log": (log_h, log_ref),
        "k": (k_h, kv),
        "ti": (ti_h, ti_ref),
        "tb": (tb_h.at[me], tb_ref),
        "v": (v_h, vv),
        "ug": (ug_h.at[0:640], ust.at[0:640]),
        "uv": (uv_h.at[0:640], ust.at[640:1280]),
        "ug2": (ug_h.at[640:704], ust.at[1280:1344]),
        "uv2": (uv_h.at[640:704], ust.at[1344:1408]),
        "q": (q_h, qv),
        "g": (g_h, gv),
        "ow": (ow_h, owv),
        "dw": (dw_h, wd.at[0:FF, pl.ds(pl.multiple_of(me * 128, 128), 128)]),
        "res": (res_h.at[pl.ds(pl.multiple_of(t * 128, 128), 128)], rv),
        "gain": (gain_h, gain_ref),
        "bias": (bias_h, bias_ref),
        "taps": (taps_h, taps_ref),
        "shift": (shift_h, shift_ref),
    }
    loads = {
        name: pltpu.make_async_copy(src, dst, in_sem.at[5 if i in (6, 7, 8) else i])
        for i, (name, (src, dst)) in enumerate(loads.items())
    }
    for load in loads.values():
        load.start()

    def loaded(*names):
        for name in names:
            loads[name].wait()

    barrier = pltpu.get_barrier_semaphore()

    def sp_peer(i):
        j = lax.rem(me + i, NSP)
        return j, {"z": lax.div(j, 4), "y": lax.rem(j, 4)}

    def greet(i, carry):
        _, dev = sp_peer(i)
        pl.semaphore_signal(barrier, inc=1, device_id=dev, device_id_type=MESH)
        return carry

    lax.fori_loop(1, NSP, greet, 0)
    for dev in (SIB, XR, XL):
        pl.semaphore_signal(barrier, inc=1, device_id=dev, device_id_type=MESH)

    yr, yl, yo = lax.rem(y + 1, 4), lax.rem(y + 3, 4), lax.rem(y + 2, 4)
    zr, zl, zo = lax.rem(z + 1, 4), lax.rem(z + 3, 4), lax.rem(z + 2, 4)
    YR, YL, ZR, ZL = at("y", yr), at("y", yl), at("z", zr), at("z", zl)

    def up_piece(zz, yy, lo, n):
        return wu.at[zz * 4 + yy, lo * 16 : (lo + n) * 16, :]

    def dn_piece(zz, yy, lo, n):
        col = pl.multiple_of((zz * 4 + yy) * 128, 128)
        return wd.at[lo * 88 : (lo + n) * 88, pl.ds(col, 128)]

    def gather(g, piece, bytes_of):
        def put(n, zz, yy, lo, cnt, dev):
            p = piece(zz, yy, lo, cnt)
            remote(p, p, wg_s.at[g], wg_r.at[g, n], dev).start()

        def got(n, shards):
            p = bytes_of(shards)
            remote(p, p, wg_s.at[g], wg_r.at[g, n], YR).wait_recv()

        def s0():
            put(0, z, y, 0, 4, YR)
            put(0, z, y, 0, 4, YL)
            put(0, z, y, 4, 4, ZR)
            put(0, z, y, 4, 4, ZL)

        def s0b():
            put(2, z, y, 0, 4, ZR)
            put(2, z, y, 0, 4, ZL)
            put(2, z, y, 4, 4, YR)
            put(2, z, y, 4, 4, YL)

        def s1():
            got(0, 2)
            put(1, z, yl, 0, 2, YR)
            put(1, z, yr, 2, 2, YL)
            put(1, zl, y, 4, 2, ZR)
            put(1, zr, y, 6, 2, ZL)
            put(3, z, yl, 0, 4, ZR)
            put(3, z, yl, 0, 4, ZL)
            put(3, zl, y, 4, 4, YR)
            put(3, zl, y, 4, 4, YL)
            put(4, z, yr, 0, 4, ZR)
            put(4, z, yr, 0, 4, ZL)
            put(4, zr, y, 4, 4, YR)
            put(4, zr, y, 4, 4, YL)

        def s2():
            got(1, 1)
            put(5, z, yo, 0, 4, ZR)
            put(5, z, yo, 0, 4, ZL)
            put(5, zo, y, 4, 4, YR)
            put(5, zo, y, 4, 4, YL)

        def s3(m):
            ym, zm = (y, yl, yr, yo)[m], (z, zl, zr, zo)[m]
            got(2 + m, 2)
            put(6, zl, ym, 0, 2, ZR)
            put(6, zr, ym, 2, 2, ZL)
            put(6, zm, yl, 4, 2, YR)
            put(6, zm, yr, 6, 2, YL)

        def s4():
            got(6, 4)

        def drain():
            p = bytes_of(15)
            remote(p, p, wg_s.at[g], wg_r.at[g, 0], YR).wait_send()

        return s0, s0b, s1, s2, s3, s4, drain

    u0, u0b, u1, u2, u3, u4, udrain = gather(0, up_piece, lambda n: wu.at[0:n])
    n0, n0b, n1, n2, n3, n4, ndrain = gather(1, dn_piece, lambda n: wd.at[0:FF, 0 : n * 128])

    ri = lax.broadcasted_iota(jnp.int32, (BLK, BLK), 0)
    ci = lax.broadcasted_iota(jnp.int32, (BLK, BLK), 1)
    causal = ri >= ci
    tri = jnp.where(causal, 1.0, 0.0).astype(F32)
    lsc[...] = jnp.zeros((8, 256), F32)
    loaded("log")
    for b in range(4):
        lsc[b : b + 1, 0:128] = log_ref[2 * b : 2 * b + 1, :]
        lsc[b : b + 1, 128:256] = log_ref[2 * b + 1 : 2 * b + 2, :]
    logs = lsc[...]
    crow[...] = lax.dot_general(logs, tri, NT, precision=HIGH, preferred_element_type=F32)
    ccol[...] = lax.dot_general(tri, logs, NT, precision=HIGH, preferred_element_type=F32)
    loaded("k", "ti", "tb", "v")
    base = tb_ref[...]

    def turned(ref, b):
        ci_, si_ = ti_ref[0], ti_ref[1]
        cb_, sb_ = base[b : b + 1, :], base[4 + b : 5 + b, :]
        cos = cb_ * ci_ - sb_ * si_
        sin = sb_ * ci_ + cb_ * si_
        front = ref[b * BLK : (b + 1) * BLK, 0:128].astype(F32)
        second = ref[b * BLK : (b + 1) * BLK, 128:256].astype(F32)
        return front * cos - second * sin, front * sin + second * cos

    decay = jnp.ones((1, 1), F32)
    for b in range(4):
        front, second = turned(kv, b)
        front = (front * 0.0625).astype(BF16)
        second = (second * 0.0625).astype(BF16)
        kr[b, :, 0:128] = front
        kr[b, :, 128:256] = second
        total = crow[b : b + 1, 255:256]
        to_end = jnp.exp(total - ccol[:, b : b + 1])
        faded = jnp.concatenate([front, second], axis=1).astype(F32) * to_end
        state = lax.dot_general(
            faded.astype(BF16), vv[b * BLK : (b + 1) * BLK, :], TN, preferred_element_type=F32
        )
        step = jnp.exp(total)
        dpre[b] = jnp.broadcast_to(decay, (8, 128))
        decay = decay * step
        if b == 0:
            loc[b] = jnp.zeros((BLK, 512), F32)
            loc[b + 1] = state
        else:
            loc[b + 1] = step * loc[b] + state

    hi = decay.astype(BF16)
    mid = (decay - hi.astype(F32)).astype(BF16)
    low = (decay - hi.astype(F32) - mid.astype(F32)).astype(BF16)
    row = lax.broadcasted_iota(jnp.int32, (16, 128), 0)
    tag = jnp.where(
        row == 0,
        hi.astype(F32),
        jnp.where(row == 1, mid.astype(F32), jnp.where(row == 2, low.astype(F32), 0.0)),
    ).astype(BF16)
    for j in range(NSP):
        ssend[j, :, 0:512] = loc[4, j * 16 : (j + 1) * 16, :].astype(BF16)
        ssend[j, :, 512:640] = tag

    pl.semaphore_wait(barrier, NSP + 2)

    def scatter(i, carry):
        j, dev = sp_peer(i)
        remote(ssend.at[j], srecv.at[me], st_s.at[0], st_r.at[0], dev).start()
        return carry

    lax.fori_loop(1, NSP, scatter, 0)
    srecv[me] = ssend[me]

    pltpu.make_async_copy(ust, ust, in_sem.at[5]).wait()
    for n in range(11):
        tile = ust[n * 128 : (n + 1) * 128, :].astype(F32)
        wu[me, :, n * 128 : (n + 1) * 128] = tile.T.astype(BF16)
    u0()

    loaded("q")
    for b in range(4):
        front, second = turned(qv, b)
        qr = jnp.concatenate([front, second], axis=1).astype(BF16)
        column = ccol[:, b : b + 1]
        sq[b] = (qr.astype(F32) * jnp.exp(column)).astype(BF16)
        scores = lax.dot_general(qr, kr[b], NT, preferred_element_type=F32)
        gap = column - crow[b : b + 1, :]
        weight = jnp.where(causal, jnp.exp(jnp.where(causal, gap, 0.0)), 0.0)
        within[b] = jnp.dot(
            (scores * weight).astype(BF16),
            vv[b * BLK : (b + 1) * BLK, :],
            preferred_element_type=F32,
        )
    wd[FF:FFP, :] = jnp.zeros((FFP - FF, 2048), BF16)
    act0[:, :, FF:FFP] = jnp.zeros((4, 128, FFP - FF), BF16)
    act1[:, :, FF:FFP] = jnp.zeros((4, 128, FFP - FF), BF16)

    fifteen = slice(0, NSP - 1)
    scattered = remote(ssend.at[fifteen], srecv.at[fifteen], st_s.at[0], st_r.at[0], YR)
    returned = remote(rsend.at[fifteen], inc.at[fifteen], st_s.at[1], st_r.at[1], YR)
    scattered.wait_recv()
    acc = jnp.zeros((16, 512), F32)
    for d in range(NSP):
        rsend[d] = acc.astype(BF16)
        if d < NSP - 1:
            tags = srecv[d, :, 512:640].astype(F32)
            factor = tags[0:1, 0:1] + tags[1:2, 0:1] + tags[2:3, 0:1]
            acc = factor * acc + srecv[d, :, 0:512].astype(F32)
    inc[me] = rsend[me]

    def give_back(i, carry):
        j, dev = sp_peer(i)
        remote(rsend.at[j], inc.at[me], st_s.at[1], st_r.at[1], dev).start()
        return carry

    lax.fori_loop(1, NSP, give_back, 0)
    u0b()
    u1()

    returned.wait_recv()

    order = (xo, xr, xl, x)
    L, R = slice(0, 1024), slice(1024, 2048)

    class Scatter:
        def __init__(self, s, h):
            self.s, self.h = s, h
            self.lo, self.hi = ROWS[s][h]
            rows = slice(self.lo, self.hi)

            def across(n, src, dst, dev):
                return remote(src, dst, x_s.at[s, h], x_r.at[s, h, n], dev)

            self.a_out = across(0, cb.at[s, 0, rows, L], ra.at[s, rows], XR)
            self.b_out = across(1, cb.at[s, 0, rows, R], rb.at[s, rows], XL)
            self.r_late = across(2, cb.at[s, 1, rows, L], rl.at[s, rows, L], XR)
            self.r_soon = across(2, cb.at[s, 1, rows, R], rl.at[s, rows, R], XR)
            self.l_soon = across(2, cb.at[s, 2, rows, L], rr.at[s, rows, L], XL)
            self.l_late = across(2, cb.at[s, 2, rows, R], rr.at[s, rows, R], XL)
            self.into = across(2, cb.at[s, 0:2, rows], d2.at[s, 0:2, rows], XR)
            self.away = across(2, cb.at[s, 0:3, rows], d2.at[s, 0:3, rows], XR)

        def pair(self, j):
            s, h, rows = self.s, self.h, slice(self.lo, self.hi)
            return remote(
                part.at[s, j, 1 - c, rows], d2.at[s, j, rows], d2_s.at[s, h], d2_r.at[s, h, j], SIB
            )

        def merged(self, j, cols, extra=None):
            s = self.s

            for r in self.steps():
                v = part[s, j, c, r, cols].astype(F32) + d2[s, j, r, cols].astype(F32)
                if extra is not None:
                    v = v + extra[s, r, :].astype(F32)
                cb[s, j, r, cols] = v.astype(BF16)

        def steps(self):
            return [slice(r, min(r + 32, self.hi)) for r in range(self.lo, self.hi, 32)]

        def far(self):
            self.pair(0).wait_recv()
            self.merged(0, L)
            self.a_out.start()
            self.merged(0, R)
            self.b_out.start()

        def soon_right(self):
            self.pair(1).wait_recv()
            self.merged(1, R)
            self.r_soon.start()

        def soon_left(self):
            self.pair(2).wait_recv()
            self.merged(2, L)
            self.l_soon.start()

        def late(self):
            self.a_out.wait_recv()
            self.merged(1, L, ra)
            self.r_late.start()
            self.b_out.wait_recv()
            self.merged(2, R, rb)
            self.l_late.start()

        def finish(self):
            self.pair(3).wait_recv()
            self.into.wait_recv()

        def each(self, step):
            for r in self.steps():
                step(r)

        def drain(self):
            s, h, rows = self.s, self.h, slice(self.lo, self.hi)
            remote(
                d2.at[s, :, rows], d2.at[s, :, rows], d2_s.at[s, h], d2_r.at[s, h, 0], SIB
            ).wait_send()
            self.away.wait_send()

    def summed(s, r):
        v = part[s, 3, c, r, :].astype(F32) + d2[s, 3, r, :].astype(F32)
        return v + rl[s, r, :].astype(F32) + rr[s, r, :].astype(F32)

    def normed(v, i):
        mean = jnp.mean(v, axis=-1, keepdims=True)
        v = v - mean
        var = jnp.mean(v * v, axis=-1, keepdims=True)
        return v * lax.rsqrt(var + EPS) * gain_ref[i : i + 1, :] + bias_ref[i : i + 1, :]

    loaded("g", "ow")

    def mix(b):
        rows = pl.ds(pl.multiple_of(b * BLK, BLK), BLK)
        state = dpre[b][0:1, 0:1] * inc[...].reshape(BLK, 512).astype(F32) + loc[b]
        mixed = within[b] + jnp.dot(sq[b], state.astype(BF16), preferred_element_type=F32)
        mean = jnp.mean(mixed, axis=-1, keepdims=True)
        mixed = mixed - mean
        var = jnp.mean(mixed * mixed, axis=-1, keepdims=True)
        mixed = mixed * lax.rsqrt(var + EPS)
        gate = gv[rows, :].astype(F32)
        gr[...] = (gate * jax.nn.sigmoid(gate) * mixed).astype(BF16).reshape(2, 128, 512)

    def project(j, lo=0, hi=128):
        def tile(n, carry):
            cols = pl.ds(pl.multiple_of(n * 512, 512), 512)
            lhs = gr[:, lo:hi].reshape(2 * (hi - lo), 512)
            p = jnp.dot(lhs, owv[:, cols], preferred_element_type=F32)
            part[0, j, :, lo:hi, cols] = p.astype(BF16).reshape(2, hi - lo, 512)
            return carry

        lax.fori_loop(0, 4, tile, 0)

    A = [Scatter(0, 0), Scatter(0, 1)]
    mix(order[0])
    for h in A:
        project(0, h.lo, h.hi)
        h.pair(0).start()
    mix(order[1])
    A[0].far()
    project(1)
    for h in A:
        h.pair(1).start()
    mix(order[2])
    project(2)
    for h in A:
        h.pair(2).start()
    A[0].soon_right()
    A[1].far()
    mix(order[3])
    project(3)
    for h in A:
        h.pair(3).start()
    A[0].soon_left()
    A[0].late()
    A[1].soon_right()
    A[1].soon_left()
    u2()
    u3(0)
    u3(1)
    u3(2)
    loaded("dw")
    n0()
    n0b()
    A[1].late()
    u3(3)
    loaded("res", "gain", "bias")

    def first_norm(r):
        v = ALPHA * rv[r, :].astype(F32) + summed(0, r)
        xb[t, r, :] = normed(v, 0).astype(BF16)

    tl, tr, to = xl * 2 + c, xr * 2 + c, xo * 2 + c
    W = slice(0, 2048)

    def ag(h, n, owner, cols, dev):
        lo, hi = ROWS[0][h]
        p = xb.at[owner, lo:hi, cols]
        return remote(p, p, ag_s.at[h], ag_r.at[h, n], dev)

    def go(h, n, owner, cols, dev):
        ag(h, n, owner, cols, dev).start()

    def several(h, n, owners):
        lo, hi = ROWS[0][h]
        p = xb.at[0:owners, lo:hi]
        return remote(p, p, ag_s.at[h], ag_r.at[h, n], SIB)

    def arrived(h, n, owner, cols):
        ag(h, n, owner, cols, SIB).wait_recv()

    def own_rows(h):
        go(h, 1, t, L, XR)
        go(h, 3, t, R, XL)
        if h == 0:
            go(h, 0, t, W, SIB)
        go(h, 2, t, R, XR)
        go(h, 4, t, L, XL)

    def pass_on(h):
        arrived(h, 1, tl, L)
        go(h, 5, tl, L, XR)
        arrived(h, 3, tr, R)
        go(h, 6, tr, R, XL)
        go(h, 7, tl, L, SIB)
        go(h, 7, tr, R, SIB)

    def pass_second(h):
        arrived(h, 2, tl, R)
        go(h, 7, tl, R, SIB)
        arrived(h, 4, tr, L)
        go(h, 7, tr, L, SIB)

    def near_ready(h):
        several(h, 7, 2).wait_recv()

    def pass_far(h):
        arrived(h, 5, to, L)
        go(h, 8, to, L, SIB)
        arrived(h, 6, to, R)
        go(h, 8, to, R, SIB)

    def far_ready(h):
        several(h, 8, 1).wait_recv()

    def up(*items):
        def cols_of(cols, width):
            lhs = []
            for h, b in items:
                lo, hi = ROWS[0][h]
                lhs.append(xb[pl.ds(2 * b, 2), lo:hi].reshape(2 * (hi - lo), 2048))
            lhs = lhs[0] if len(lhs) == 1 else jnp.concatenate(lhs, axis=0)
            w = wu[:, :, cols].reshape(2048, width)
            out = jnp.dot(lhs, w, preferred_element_type=F32).astype(BF16)
            k = 0
            for h, b in items:
                lo, hi = ROWS[0][h]
                for d in range(2):
                    at_row = pl.multiple_of(16 + (2 * b + d) * 128 + lo, 16)
                    ub[pl.ds(at_row, hi - lo), cols] = out[k : k + hi - lo]
                    k += hi - lo

        def tile(n, carry):
            cols_of(pl.ds(pl.multiple_of(n * 256, 256), 256), 256)
            return carry

        lax.fori_loop(0, 5, tile, 0)
        cols_of(slice(1280, 1408), 128)

    def halo_copy():
        nxt = lax.rem(me + 1, NSP)
        dev = {"z": lax.div(nxt, 4), "y": lax.rem(nxt, 4)}
        return remote(ub.at[1024:1040, :], halo, h_s.at[0], h_r.at[0], dev)

    def send_halo(when):
        @pl.when(jnp.logical_and(when, me < NSP - 1))
        def _():
            halo_copy().start()

    @pl.when(me == 0)
    def _():
        ub[0:16, :] = jnp.zeros((16, 1408), BF16)

    def conv(g, b):
        lo, hi = ROWS[1][g]
        n_rows = hi - lo
        act = (act0, act1)[g]

        def three(block, half, lanes):
            v = shift_ref[half : half + 1, lanes] + block[14 : 14 + n_rows] * taps_ref[0, half : half + 1, lanes]
            v = v + block[15 : 15 + n_rows] * taps_ref[1, half : half + 1, lanes]
            return v + block[16 : 16 + n_rows] * taps_ref[2, half : half + 1, lanes]

        def device(d, carry):
            around = pl.ds(pl.multiple_of((2 * b + d) * 128 + lo, 16), n_rows + 16)
            rows = pl.ds(pl.multiple_of(d * n_rows, 16), n_rows)
            for n in range(6):
                if n < 5:
                    lanes = slice(n * 128, (n + 1) * 128)
                    gate = ub[around, lanes].astype(F32)
                    value = ub[around, 640 + n * 128 : 640 + (n + 1) * 128].astype(F32)
                else:
                    lanes = slice(640, FF)
                    both = ub[around, 1280:1408].astype(F32)
                    gate, value = both[:, 0:64], pltpu.roll(both, 64, 1)[:, 0:64]
                a = jax.nn.gelu(three(gate, 0, lanes)) * three(value, 1, lanes)
                act[b, rows, lanes] = a.astype(BF16)
            return carry

        lax.fori_loop(0, 2, device, 0)

    def down(g, js, chips):
        lo, hi = ROWS[1][g]
        act = (act0, act1)[g]

        def tile(n, carry):
            cols = pl.ds(pl.multiple_of(n * 512, 512), 512)
            lhs = [act[b] for b in chips]
            lhs = lhs[0] if len(lhs) == 1 else jnp.concatenate(lhs, axis=0)
            p = jnp.dot(lhs, wd[:, cols], preferred_element_type=F32).astype(BF16)
            p = p.reshape(len(js), 2, hi - lo, 512)
            for i, j in enumerate(js):
                part[1, j, :, lo:hi, cols] = p[i]
            return carry

        lax.fori_loop(0, 4, tile, 0)

    B = [Scatter(1, 0), Scatter(1, 1)]
    A[0].finish()
    A[0].each(first_norm)
    own_rows(0)
    A[1].finish()
    A[1].each(first_norm)
    go(1, 0, t, W, SIB)
    n1()
    pass_on(0)
    own_rows(1)
    u4()
    loaded("taps", "shift")
    arrived(0, 0, t + 1 - 2 * c, W)
    arrived(1, 0, t + 1 - 2 * c, W)
    up((0, x), (1, x))
    send_halo(x == 3)
    pass_second(0)
    n2()
    n3(0)
    conv(0, x)
    near_ready(0)
    n3(1)
    up((0, xr), (0, xl))
    send_halo(jnp.logical_or(xr == 3, xl == 3))
    pass_far(0)
    n3(2)
    conv(0, xr)
    conv(0, xl)
    pass_on(1)
    n3(3)
    far_ready(0)
    up((0, xo))
    send_halo(xo == 3)
    pass_second(1)
    conv(0, xo)
    n4()
    down(0, (0,), (xo,))
    B[0].pair(0).start()
    down(0, (1, 2), (xr, xl))
    B[0].pair(1).start()
    B[0].pair(2).start()
    pass_far(1)
    B[0].far()
    down(0, (3,), (x,))
    B[0].pair(3).start()
    B[0].soon_right()
    B[0].soon_left()
    near_ready(1)
    far_ready(1)
    up((1, xo), (1, xr), (1, xl))

    @pl.when(me > 0)
    def _():
        halo_copy().wait_recv()
        ub[0:16, :] = halo[...]

    conv(1, xo)
    down(1, (0,), (xo,))
    B[1].pair(0).start()
    B[0].late()
    conv(1, xr)
    down(1, (1,), (xr,))
    B[1].pair(1).start()
    B[1].far()
    conv(1, xl)
    down(1, (2,), (xl,))
    B[1].pair(2).start()
    B[1].soon_right()
    conv(1, x)
    down(1, (3,), (x,))
    B[1].pair(3).start()
    B[1].soon_left()

    def last_norm(r):
        v = ALPHA * xb[t, r, :].astype(F32) + summed(1, r)
        ov[r, :] = normed(v, 1).astype(BF16)

    outs = []
    for g in range(2):
        if g == 1:
            B[g].late()
        B[g].finish()
        B[g].each(last_norm)
        lo, hi = ROWS[1][g]
        outs.append(pltpu.make_async_copy(ov.at[lo:hi], o_ref.at[lo:hi], out_sem.at[g]))
        outs[g].start()

    scattered.wait_send()
    returned.wait_send()
    udrain()
    ndrain()
    for op in A + B:
        op.drain()
    for h in range(2):
        several(h, 0, 7).wait_send()

    @pl.when(me < NSP - 1)
    def _():
        halo_copy().wait_send()

    for op in outs:
        op.wait()


def shards(q, k, v, g, logd, res, ow, gain, bias, ug, uv, cw, cbias, dw):
    ti, tb = position_tables()
    dma = pltpu.SemaphoreType.DMA
    hb = pl.BlockSpec(memory_space=pl.ANY)
    return pl.pallas_call(
        body,
        out_shape=jax.ShapeDtypeStruct((128, 2048), BF16),
        in_specs=[hb] * 16,
        out_specs=hb,
        scratch_shapes=[
            pltpu.VMEM((1024, 256), BF16),
            pltpu.VMEM((1024, 256), BF16),
            pltpu.VMEM((1024, 512), BF16),
            pltpu.VMEM((1024, 512), BF16),
            pltpu.VMEM((8, 128), F32),
            pltpu.VMEM((128, 2048), BF16),
            pltpu.VMEM((512, 2048), BF16),
            pltpu.VMEM((2, 2048), F32),
            pltpu.VMEM((2, 2048), F32),
            pltpu.VMEM((1408, 128), BF16),
            pltpu.VMEM((3, 2, FF), F32),
            pltpu.VMEM((2, FF), F32),
            pltpu.VMEM((2, BLK, 128), F32),
            pltpu.VMEM((8, 128), F32),
            pltpu.VMEM((NSP, 128, 1408), BF16),
            pltpu.VMEM((FFP, 2048), BF16),
            pltpu.VMEM((8, 256), F32),
            pltpu.VMEM((8, 256), F32),
            pltpu.VMEM((256, 8), F32),
            pltpu.VMEM((4, 8, 128), F32),
            pltpu.VMEM((4, 256, 256), BF16),
            pltpu.VMEM((4, 256, 256), BF16),
            pltpu.VMEM((5, 256, 512), F32),
            pltpu.VMEM((4, 256, 512), F32),
            pltpu.VMEM((2, 128, 512), BF16),
            pltpu.VMEM((NSP, 16, 640), BF16),
            pltpu.VMEM((NSP, 16, 640), BF16),
            pltpu.VMEM((NSP, 16, 512), BF16),
            pltpu.VMEM((NSP, 16, 512), BF16),
            pltpu.VMEM((2, 4, 2, 128, 2048), BF16),
            pltpu.VMEM((2, 4, 128, 2048), BF16),
            pltpu.VMEM((2, 3, 128, 2048), BF16),
            pltpu.VMEM((2, 128, 1024), BF16),
            pltpu.VMEM((2, 128, 1024), BF16),
            pltpu.VMEM((2, 128, 2048), BF16),
            pltpu.VMEM((2, 128, 2048), BF16),
            pltpu.VMEM((8, 128, 2048), BF16),
            pltpu.VMEM((1040, 1408), BF16),
            pltpu.VMEM((4, 128, FFP), BF16),
            pltpu.VMEM((4, 128, FFP), BF16),
            pltpu.VMEM((16, 1408), BF16),
            pltpu.VMEM((128, 2048), BF16),
            dma((18,)),
            dma((2,)),
            dma((2,)),
            dma((2,)),
            dma((2, 7)),
            dma((2, 2)),
            dma((2, 2, 4)),
            dma((2, 2)),
            dma((2, 2, 3)),
            dma((2,)),
            dma((2, 9)),
            dma((1,)),
            dma((1,)),
            dma((2,)),
        ],
        compiler_params=pltpu.CompilerParams(
            collective_id=0, has_side_effects=True, vmem_limit_bytes=62 * 1024 * 1024
        ),
        name="layer",
    )(
        q, k, v, g, logd.reshape(8, 128), res, ow, gain, bias, ug.T, uv.T,
        cw.transpose(1, 0, 2), cbias, dw, ti, tb,
    )


def solution(mesh):
    torus = Mesh(mesh.devices.reshape(4, 4, 4, 2), ("z", "y", "x", "c"))
    sp, tp = ("z", "y"), ("x", "c")
    return jax.shard_map(
        shards,
        mesh=torus,
        in_specs=(
            P(sp, tp),
            P(sp, tp),
            P(sp, tp),
            P(sp, tp),
            P(sp, tp),
            P(sp, None),
            P(tp, None),
            P(),
            P(),
            P(sp, tp),
            P(sp, tp),
            P(None, None, tp),
            P(None, tp),
            P(tp, sp),
        ),
        out_specs=P(sp + tp, None),
        check_vma=False,
    )
```

```python
import functools

import jax
import jax.numpy as jnp
import numpy as np
from jax import lax
from jax.experimental import pallas as pl
from jax.experimental.pallas import tpu as pltpu
from jax.sharding import Mesh
from jax.sharding import PartitionSpec as P

F32 = jnp.float32
BF16 = jnp.bfloat16
HIGH = lax.Precision.HIGHEST
MESH = pl.DeviceIdType.MESH
ALPHA = 8.0**0.25
EPS = 1e-05
NSP = 16
BLK = 256
FF = 704
FFP = 768
ROWS = (((48, 128), (0, 48)), ((64, 128), (0, 64)))
NT = (((1,), (1,)), ((), ()))
TN = (((0,), (0,)), ((), ()))


def position_tables():
    freq = 10000.0 ** (-2.0 * np.arange(128, dtype=np.float64) / 256.0)
    inner = np.arange(BLK, dtype=np.float64)[:, None] * freq[None]
    start = np.arange(4 * NSP, dtype=np.float64)[:, None] * BLK * freq[None]
    ti = np.stack([np.cos(inner), np.sin(inner)]).astype(np.float32)
    tb = np.concatenate(
        [np.cos(start).reshape(NSP, 4, 128), np.sin(start).reshape(NSP, 4, 128)], axis=1
    ).astype(np.float32)
    return ti, tb


def body(
    q_h, k_h, v_h, g_h, log_h, res_h, ow_h, gain_h, bias_h, ug_h, uv_h, taps_h, shift_h, dw_h,
    ti_h, tb_h, o_ref,
    qv, kv, vv, gv, log_ref, rv, owv, gain_ref, bias_ref, ust, taps_ref, shift_ref, ti_ref, tb_ref,
    wu, wd,
    lsc, crow, ccol, dpre, kr, sq, loc, within, gr,
    ssend, srecv, rsend, inc,
    part, d2, cb, ra, rb, rl, rr,
    xb, ub, act0, act1, halo, ov,
    in_sem, st_s, st_r, wg_s, wg_r, d2_s, d2_r, x_s, x_r, ag_s, ag_r, h_s, h_r, out_sem,
):
    z, y, x, c = (lax.axis_index(a) for a in ("z", "y", "x", "c"))
    me = z * 4 + y
    t = x * 2 + c
    xr, xl, xo = lax.rem(x + 1, 4), lax.rem(x + 3, 4), lax.rem(x + 2, 4)

    def at(axis, value):
        return {axis: value}

    SIB = at("c", 1 - c)
    XR, XL = at("x", xr), at("x", xl)

    def remote(src, dst, ssem, rsem, dev):
        return pltpu.make_async_remote_copy(
            src_ref=src, dst_ref=dst, send_sem=ssem, recv_sem=rsem, device_id=dev,
            device_id_type=MESH,
        )

    loads = {
        "log": (log_h, log_ref),
        "k": (k_h, kv),
        "ti": (ti_h, ti_ref),
        "tb": (tb_h.at[me], tb_ref),
        "v": (v_h, vv),
        "ug": (ug_h.at[0:640], ust.at[0:640]),
        "uv": (uv_h.at[0:640], ust.at[640:1280]),
        "ug2": (ug_h.at[640:704], ust.at[1280:1344]),
        "uv2": (uv_h.at[640:704], ust.at[1344:1408]),
        "q": (q_h, qv),
        "g": (g_h, gv),
        "ow": (ow_h, owv),
        "dw": (dw_h, wd.at[0:FF, pl.ds(pl.multiple_of(me * 128, 128), 128)]),
        "res": (res_h.at[pl.ds(pl.multiple_of(t * 128, 128), 128)], rv),
        "gain": (gain_h, gain_ref),
        "bias": (bias_h, bias_ref),
        "taps": (taps_h, taps_ref),
        "shift": (shift_h, shift_ref),
    }
    loads = {
        name: pltpu.make_async_copy(src, dst, in_sem.at[5 if i in (6, 7, 8) else i])
        for i, (name, (src, dst)) in enumerate(loads.items())
    }
    for load in loads.values():
        load.start()

    def loaded(*names):
        for name in names:
            loads[name].wait()

    barrier = pltpu.get_barrier_semaphore()

    def sp_peer(i):
        j = lax.rem(me + i, NSP)
        return j, {"z": lax.div(j, 4), "y": lax.rem(j, 4)}

    def greet(i, carry):
        _, dev = sp_peer(i)
        pl.semaphore_signal(barrier, inc=1, device_id=dev, device_id_type=MESH)
        return carry

    lax.fori_loop(1, NSP, greet, 0)
    for dev in (SIB, XR, XL):
        pl.semaphore_signal(barrier, inc=1, device_id=dev, device_id_type=MESH)

    yr, yl, yo = lax.rem(y + 1, 4), lax.rem(y + 3, 4), lax.rem(y + 2, 4)
    zr, zl, zo = lax.rem(z + 1, 4), lax.rem(z + 3, 4), lax.rem(z + 2, 4)
    YR, YL, ZR, ZL = at("y", yr), at("y", yl), at("z", zr), at("z", zl)

    def up_piece(zz, yy, lo, n):
        return wu.at[zz * 4 + yy, lo * 16 : (lo + n) * 16, :]

    def dn_piece(zz, yy, lo, n):
        col = pl.multiple_of((zz * 4 + yy) * 128, 128)
        return wd.at[lo * 88 : (lo + n) * 88, pl.ds(col, 128)]

    def gather(g, piece, bytes_of):
        def put(n, zz, yy, lo, cnt, dev):
            p = piece(zz, yy, lo, cnt)
            remote(p, p, wg_s.at[g], wg_r.at[g, n], dev).start()

        def got(n, shards):
            p = bytes_of(shards)
            remote(p, p, wg_s.at[g], wg_r.at[g, n], YR).wait_recv()

        def s0():
            put(0, z, y, 0, 4, YR)
            put(0, z, y, 0, 4, YL)
            put(0, z, y, 4, 4, ZR)
            put(0, z, y, 4, 4, ZL)

        def s0b():
            put(2, z, y, 0, 4, ZR)
            put(2, z, y, 0, 4, ZL)
            put(2, z, y, 4, 4, YR)
            put(2, z, y, 4, 4, YL)

        def s1():
            got(0, 2)
            put(1, z, yl, 0, 2, YR)
            put(1, z, yr, 2, 2, YL)
            put(1, zl, y, 4, 2, ZR)
            put(1, zr, y, 6, 2, ZL)
            put(3, z, yl, 0, 4, ZR)
            put(3, z, yl, 0, 4, ZL)
            put(3, zl, y, 4, 4, YR)
            put(3, zl, y, 4, 4, YL)
            put(4, z, yr, 0, 4, ZR)
            put(4, z, yr, 0, 4, ZL)
            put(4, zr, y, 4, 4, YR)
            put(4, zr, y, 4, 4, YL)

        def s2():
            got(1, 1)
            put(5, z, yo, 0, 4, ZR)
            put(5, z, yo, 0, 4, ZL)
            put(5, zo, y, 4, 4, YR)
            put(5, zo, y, 4, 4, YL)

        def s3(m):
            ym, zm = (y, yl, yr, yo)[m], (z, zl, zr, zo)[m]
            got(2 + m, 2)
            put(6, zl, ym, 0, 2, ZR)
            put(6, zr, ym, 2, 2, ZL)
            put(6, zm, yl, 4, 2, YR)
            put(6, zm, yr, 6, 2, YL)

        def s4():
            got(6, 4)

        def drain():
            p = bytes_of(15)
            remote(p, p, wg_s.at[g], wg_r.at[g, 0], YR).wait_send()

        return s0, s0b, s1, s2, s3, s4, drain

    u0, u0b, u1, u2, u3, u4, udrain = gather(0, up_piece, lambda n: wu.at[0:n])
    n0, n0b, n1, n2, n3, n4, ndrain = gather(1, dn_piece, lambda n: wd.at[0:FF, 0 : n * 128])

    ri = lax.broadcasted_iota(jnp.int32, (BLK, BLK), 0)
    ci = lax.broadcasted_iota(jnp.int32, (BLK, BLK), 1)
    causal = ri >= ci
    tri = jnp.where(causal, 1.0, 0.0).astype(F32)
    lsc[...] = jnp.zeros((8, 256), F32)
    loaded("log")
    for b in range(4):
        lsc[b : b + 1, 0:128] = log_ref[2 * b : 2 * b + 1, :]
        lsc[b : b + 1, 128:256] = log_ref[2 * b + 1 : 2 * b + 2, :]
    logs = lsc[...]
    crow[...] = lax.dot_general(logs, tri, NT, precision=HIGH, preferred_element_type=F32)
    ccol[...] = lax.dot_general(tri, logs, NT, precision=HIGH, preferred_element_type=F32)
    loaded("k", "ti", "tb", "v")
    base = tb_ref[...]

    def turned(ref, b):
        ci_, si_ = ti_ref[0], ti_ref[1]
        cb_, sb_ = base[b : b + 1, :], base[4 + b : 5 + b, :]
        cos = cb_ * ci_ - sb_ * si_
        sin = sb_ * ci_ + cb_ * si_
        front = ref[b * BLK : (b + 1) * BLK, 0:128].astype(F32)
        second = ref[b * BLK : (b + 1) * BLK, 128:256].astype(F32)
        return front * cos - second * sin, front * sin + second * cos

    decay = jnp.ones((1, 1), F32)
    for b in range(4):
        front, second = turned(kv, b)
        front = (front * 0.0625).astype(BF16)
        second = (second * 0.0625).astype(BF16)
        kr[b, :, 0:128] = front
        kr[b, :, 128:256] = second
        total = crow[b : b + 1, 255:256]
        to_end = jnp.exp(total - ccol[:, b : b + 1])
        faded = jnp.concatenate([front, second], axis=1).astype(F32) * to_end
        state = lax.dot_general(
            faded.astype(BF16), vv[b * BLK : (b + 1) * BLK, :], TN, preferred_element_type=F32
        )
        step = jnp.exp(total)
        dpre[b] = jnp.broadcast_to(decay, (8, 128))
        decay = decay * step
        if b == 0:
            loc[b] = jnp.zeros((BLK, 512), F32)
            loc[b + 1] = state
        else:
            loc[b + 1] = step * loc[b] + state

    hi = decay.astype(BF16)
    mid = (decay - hi.astype(F32)).astype(BF16)
    low = (decay - hi.astype(F32) - mid.astype(F32)).astype(BF16)
    row = lax.broadcasted_iota(jnp.int32, (16, 128), 0)
    tag = jnp.where(
        row == 0,
        hi.astype(F32),
        jnp.where(row == 1, mid.astype(F32), jnp.where(row == 2, low.astype(F32), 0.0)),
    ).astype(BF16)
    for j in range(NSP):
        ssend[j, :, 0:512] = loc[4, j * 16 : (j + 1) * 16, :].astype(BF16)
        ssend[j, :, 512:640] = tag

    pl.semaphore_wait(barrier, NSP + 2)

    def scatter(i, carry):
        j, dev = sp_peer(i)
        remote(ssend.at[j], srecv.at[me], st_s.at[0], st_r.at[0], dev).start()
        return carry

    lax.fori_loop(1, NSP, scatter, 0)
    srecv[me] = ssend[me]

    pltpu.make_async_copy(ust, ust, in_sem.at[5]).wait()
    for n in range(11):
        tile = ust[n * 128 : (n + 1) * 128, :].astype(F32)
        wu[me, :, n * 128 : (n + 1) * 128] = tile.T.astype(BF16)
    u0()

    loaded("q")
    for b in range(4):
        front, second = turned(qv, b)
        qr = jnp.concatenate([front, second], axis=1).astype(BF16)
        column = ccol[:, b : b + 1]
        sq[b] = (qr.astype(F32) * jnp.exp(column)).astype(BF16)
        scores = lax.dot_general(qr, kr[b], NT, preferred_element_type=F32)
        gap = column - crow[b : b + 1, :]
        weight = jnp.where(causal, jnp.exp(jnp.where(causal, gap, 0.0)), 0.0)
        within[b] = jnp.dot(
            (scores * weight).astype(BF16),
            vv[b * BLK : (b + 1) * BLK, :],
            preferred_element_type=F32,
        )
    wd[FF:FFP, :] = jnp.zeros((FFP - FF, 2048), BF16)
    act0[:, :, FF:FFP] = jnp.zeros((4, 128, FFP - FF), BF16)
    act1[:, :, FF:FFP] = jnp.zeros((4, 128, FFP - FF), BF16)

    fifteen = slice(0, NSP - 1)
    scattered = remote(ssend.at[fifteen], srecv.at[fifteen], st_s.at[0], st_r.at[0], YR)
    returned = remote(rsend.at[fifteen], inc.at[fifteen], st_s.at[1], st_r.at[1], YR)
    scattered.wait_recv()
    acc = jnp.zeros((16, 512), F32)
    for d in range(NSP):
        rsend[d] = acc.astype(BF16)
        if d < NSP - 1:
            tags = srecv[d, :, 512:640].astype(F32)
            factor = tags[0:1, 0:1] + tags[1:2, 0:1] + tags[2:3, 0:1]
            acc = factor * acc + srecv[d, :, 0:512].astype(F32)
    inc[me] = rsend[me]

    def give_back(i, carry):
        j, dev = sp_peer(i)
        remote(rsend.at[j], inc.at[me], st_s.at[1], st_r.at[1], dev).start()
        return carry

    lax.fori_loop(1, NSP, give_back, 0)
    u0b()
    u1()

    returned.wait_recv()

    order = (xo, xr, xl, x)
    L, R = slice(0, 1024), slice(1024, 2048)

    class Scatter:
        def __init__(self, s, h):
            self.s, self.h = s, h
            self.lo, self.hi = ROWS[s][h]
            rows = slice(self.lo, self.hi)

            def across(n, src, dst, dev):
                return remote(src, dst, x_s.at[s, h], x_r.at[s, h, n], dev)

            self.a_out = across(0, cb.at[s, 0, rows, L], ra.at[s, rows], XR)
            self.b_out = across(1, cb.at[s, 0, rows, R], rb.at[s, rows], XL)
            self.r_late = across(2, cb.at[s, 1, rows, L], rl.at[s, rows, L], XR)
            self.r_soon = across(2, cb.at[s, 1, rows, R], rl.at[s, rows, R], XR)
            self.l_soon = across(2, cb.at[s, 2, rows, L], rr.at[s, rows, L], XL)
            self.l_late = across(2, cb.at[s, 2, rows, R], rr.at[s, rows, R], XL)
            self.into = across(2, cb.at[s, 0:2, rows], d2.at[s, 0:2, rows], XR)
            self.away = across(2, cb.at[s, 0:3, rows], d2.at[s, 0:3, rows], XR)

        def pair(self, j):
            s, h, rows = self.s, self.h, slice(self.lo, self.hi)
            return remote(
                part.at[s, j, 1 - c, rows], d2.at[s, j, rows], d2_s.at[s, h], d2_r.at[s, h, j], SIB
            )

        def merged(self, j, cols, extra=None):
            s = self.s

            for r in self.steps():
                v = part[s, j, c, r, cols].astype(F32) + d2[s, j, r, cols].astype(F32)
                if extra is not None:
                    v = v + extra[s, r, :].astype(F32)
                cb[s, j, r, cols] = v.astype(BF16)

        def steps(self):
            return [slice(r, min(r + 32, self.hi)) for r in range(self.lo, self.hi, 32)]

        def far(self):
            self.pair(0).wait_recv()
            self.merged(0, L)
            self.a_out.start()
            self.merged(0, R)
            self.b_out.start()

        def soon_right(self):
            self.pair(1).wait_recv()
            self.merged(1, R)
            self.r_soon.start()

        def soon_left(self):
            self.pair(2).wait_recv()
            self.merged(2, L)
            self.l_soon.start()

        def late(self):
            self.a_out.wait_recv()
            self.merged(1, L, ra)
            self.r_late.start()
            self.b_out.wait_recv()
            self.merged(2, R, rb)
            self.l_late.start()

        def finish(self):
            self.pair(3).wait_recv()
            self.into.wait_recv()

        def each(self, step):
            for r in self.steps():
                step(r)

        def drain(self):
            s, h, rows = self.s, self.h, slice(self.lo, self.hi)
            remote(
                d2.at[s, :, rows], d2.at[s, :, rows], d2_s.at[s, h], d2_r.at[s, h, 0], SIB
            ).wait_send()
            self.away.wait_send()

    def summed(s, r):
        v = part[s, 3, c, r, :].astype(F32) + d2[s, 3, r, :].astype(F32)
        return v + rl[s, r, :].astype(F32) + rr[s, r, :].astype(F32)

    def normed(v, i):
        mean = jnp.mean(v, axis=-1, keepdims=True)
        v = v - mean
        var = jnp.mean(v * v, axis=-1, keepdims=True)
        return v * lax.rsqrt(var + EPS) * gain_ref[i : i + 1, :] + bias_ref[i : i + 1, :]

    loaded("g", "ow")

    def mix(b):
        rows = pl.ds(pl.multiple_of(b * BLK, BLK), BLK)
        state = dpre[b][0:1, 0:1] * inc[...].reshape(BLK, 512).astype(F32) + loc[b]
        mixed = within[b] + jnp.dot(sq[b], state.astype(BF16), preferred_element_type=F32)
        mean = jnp.mean(mixed, axis=-1, keepdims=True)
        mixed = mixed - mean
        var = jnp.mean(mixed * mixed, axis=-1, keepdims=True)
        mixed = mixed * lax.rsqrt(var + EPS)
        gate = gv[rows, :].astype(F32)
        gr[...] = (gate * jax.nn.sigmoid(gate) * mixed).astype(BF16).reshape(2, 128, 512)

    def project(j, lo=0, hi=128):
        def tile(n, carry):
            cols = pl.ds(pl.multiple_of(n * 512, 512), 512)
            lhs = gr[:, lo:hi].reshape(2 * (hi - lo), 512)
            p = jnp.dot(lhs, owv[:, cols], preferred_element_type=F32)
            part[0, j, :, lo:hi, cols] = p.astype(BF16).reshape(2, hi - lo, 512)
            return carry

        lax.fori_loop(0, 4, tile, 0)

    A = [Scatter(0, 0), Scatter(0, 1)]
    mix(order[0])
    for h in A:
        project(0, h.lo, h.hi)
        h.pair(0).start()
    mix(order[1])
    A[0].far()
    project(1)
    for h in A:
        h.pair(1).start()
    mix(order[2])
    project(2)
    for h in A:
        h.pair(2).start()
    A[0].soon_right()
    A[1].far()
    mix(order[3])
    project(3)
    for h in A:
        h.pair(3).start()
    A[0].soon_left()
    A[0].late()
    A[1].soon_right()
    A[1].soon_left()
    u2()
    u3(0)
    u3(1)
    u3(2)
    loaded("dw")
    n0()
    n0b()
    A[1].late()
    u3(3)
    loaded("res", "gain", "bias")

    def first_norm(r):
        v = ALPHA * rv[r, :].astype(F32) + summed(0, r)
        xb[t, r, :] = normed(v, 0).astype(BF16)

    tl, tr, to = xl * 2 + c, xr * 2 + c, xo * 2 + c
    W = slice(0, 2048)

    def ag(h, n, owner, cols, dev):
        lo, hi = ROWS[0][h]
        p = xb.at[owner, lo:hi, cols]
        return remote(p, p, ag_s.at[h], ag_r.at[h, n], dev)

    def go(h, n, owner, cols, dev):
        ag(h, n, owner, cols, dev).start()

    def several(h, n, owners):
        lo, hi = ROWS[0][h]
        p = xb.at[0:owners, lo:hi]
        return remote(p, p, ag_s.at[h], ag_r.at[h, n], SIB)

    def arrived(h, n, owner, cols):
        ag(h, n, owner, cols, SIB).wait_recv()

    def own_rows(h):
        go(h, 1, t, L, XR)
        go(h, 3, t, R, XL)
        if h == 0:
            go(h, 0, t, W, SIB)
        go(h, 2, t, R, XR)
        go(h, 4, t, L, XL)

    def pass_on(h):
        arrived(h, 1, tl, L)
        go(h, 5, tl, L, XR)
        arrived(h, 3, tr, R)
        go(h, 6, tr, R, XL)
        go(h, 7, tl, L, SIB)
        go(h, 7, tr, R, SIB)

    def pass_second(h):
        arrived(h, 2, tl, R)
        go(h, 7, tl, R, SIB)
        arrived(h, 4, tr, L)
        go(h, 7, tr, L, SIB)

    def near_ready(h):
        several(h, 7, 2).wait_recv()

    def pass_far(h):
        arrived(h, 5, to, L)
        go(h, 8, to, L, SIB)
        arrived(h, 6, to, R)
        go(h, 8, to, R, SIB)

    def far_ready(h):
        several(h, 8, 1).wait_recv()

    def up(*items):
        def cols_of(cols, width):
            lhs = []
            for h, b in items:
                lo, hi = ROWS[0][h]
                lhs.append(xb[pl.ds(2 * b, 2), lo:hi].reshape(2 * (hi - lo), 2048))
            lhs = lhs[0] if len(lhs) == 1 else jnp.concatenate(lhs, axis=0)
            w = wu[:, :, cols].reshape(2048, width)
            out = jnp.dot(lhs, w, preferred_element_type=F32).astype(BF16)
            k = 0
            for h, b in items:
                lo, hi = ROWS[0][h]
                for d in range(2):
                    at_row = pl.multiple_of(16 + (2 * b + d) * 128 + lo, 16)
                    ub[pl.ds(at_row, hi - lo), cols] = out[k : k + hi - lo]
                    k += hi - lo

        def tile(n, carry):
            cols_of(pl.ds(pl.multiple_of(n * 256, 256), 256), 256)
            return carry

        lax.fori_loop(0, 5, tile, 0)
        cols_of(slice(1280, 1408), 128)

    def halo_copy():
        nxt = lax.rem(me + 1, NSP)
        dev = {"z": lax.div(nxt, 4), "y": lax.rem(nxt, 4)}
        return remote(ub.at[1024:1040, :], halo, h_s.at[0], h_r.at[0], dev)

    def send_halo(when):
        @pl.when(jnp.logical_and(when, me < NSP - 1))
        def _():
            halo_copy().start()

    @pl.when(me == 0)
    def _():
        ub[0:16, :] = jnp.zeros((16, 1408), BF16)

    def conv(g, b):
        lo, hi = ROWS[1][g]
        n_rows = hi - lo
        act = (act0, act1)[g]

        def three(block, half, lanes):
            v = shift_ref[half : half + 1, lanes] + block[14 : 14 + n_rows] * taps_ref[0, half : half + 1, lanes]
            v = v + block[15 : 15 + n_rows] * taps_ref[1, half : half + 1, lanes]
            return v + block[16 : 16 + n_rows] * taps_ref[2, half : half + 1, lanes]

        def device(d, carry):
            around = pl.ds(pl.multiple_of((2 * b + d) * 128 + lo, 16), n_rows + 16)
            rows = pl.ds(pl.multiple_of(d * n_rows, 16), n_rows)
            for n in range(6):
                if n < 5:
                    lanes = slice(n * 128, (n + 1) * 128)
                    gate = ub[around, lanes].astype(F32)
                    value = ub[around, 640 + n * 128 : 640 + (n + 1) * 128].astype(F32)
                else:
                    lanes = slice(640, FF)
                    both = ub[around, 1280:1408].astype(F32)
                    gate, value = both[:, 0:64], pltpu.roll(both, 64, 1)[:, 0:64]
                a = jax.nn.gelu(three(gate, 0, lanes)) * three(value, 1, lanes)
                act[b, rows, lanes] = a.astype(BF16)
            return carry

        lax.fori_loop(0, 2, device, 0)

    def down(g, js, chips):
        lo, hi = ROWS[1][g]
        act = (act0, act1)[g]

        def tile(n, carry):
            cols = pl.ds(pl.multiple_of(n * 512, 512), 512)
            lhs = [act[b] for b in chips]
            lhs = lhs[0] if len(lhs) == 1 else jnp.concatenate(lhs, axis=0)
            p = jnp.dot(lhs, wd[:, cols], preferred_element_type=F32).astype(BF16)
            p = p.reshape(len(js), 2, hi - lo, 512)
            for i, j in enumerate(js):
                part[1, j, :, lo:hi, cols] = p[i]
            return carry

        lax.fori_loop(0, 4, tile, 0)

    B = [Scatter(1, 0), Scatter(1, 1)]
    A[0].finish()
    A[0].each(first_norm)
    own_rows(0)
    A[1].finish()
    A[1].each(first_norm)
    go(1, 0, t, W, SIB)
    n1()
    pass_on(0)
    own_rows(1)
    u4()
    loaded("taps", "shift")
    arrived(0, 0, t + 1 - 2 * c, W)
    arrived(1, 0, t + 1 - 2 * c, W)
    up((0, x), (1, x))
    send_halo(x == 3)
    pass_second(0)
    n2()
    n3(0)
    conv(0, x)
    near_ready(0)
    n3(1)
    up((0, xr), (0, xl))
    send_halo(jnp.logical_or(xr == 3, xl == 3))
    pass_far(0)
    n3(2)
    conv(0, xr)
    conv(0, xl)
    pass_on(1)
    n3(3)
    far_ready(0)
    up((0, xo))
    send_halo(xo == 3)
    pass_second(1)
    conv(0, xo)
    n4()
    down(0, (0,), (xo,))
    B[0].pair(0).start()
    down(0, (1, 2), (xr, xl))
    B[0].pair(1).start()
    B[0].pair(2).start()
    pass_far(1)
    B[0].far()
    down(0, (3,), (x,))
    B[0].pair(3).start()
    B[0].soon_right()
    B[0].soon_left()
    near_ready(1)
    far_ready(1)
    up((1, xo), (1, xr), (1, xl))

    @pl.when(me > 0)
    def _():
        halo_copy().wait_recv()
        ub[0:16, :] = halo[...]

    conv(1, xo)
    down(1, (0,), (xo,))
    B[1].pair(0).start()
    B[0].late()
    conv(1, xr)
    B[1].far()
    down(1, (1,), (xr,))
    B[1].pair(1).start()
    conv(1, xl)
    down(1, (2,), (xl,))
    B[1].pair(2).start()
    B[1].soon_right()
    conv(1, x)
    down(1, (3,), (x,))
    B[1].pair(3).start()
    B[1].soon_left()

    outs = []

    def last_norm(r):
        v = ALPHA * xb[t, r, :].astype(F32) + summed(1, r)
        ov[r, :] = normed(v, 1).astype(BF16)
        outs.append(pltpu.make_async_copy(ov.at[r], o_ref.at[r], out_sem.at[len(outs)]))
        outs[-1].start()

    for g in range(2):
        if g == 1:
            B[g].late()
        B[g].finish()
        B[g].each(last_norm)

    scattered.wait_send()
    returned.wait_send()
    udrain()
    ndrain()
    for op in A + B:
        op.drain()
    for h in range(2):
        several(h, 0, 7).wait_send()

    @pl.when(me < NSP - 1)
    def _():
        halo_copy().wait_send()

    for op in outs:
        op.wait()


def shards(q, k, v, g, logd, res, ow, gain, bias, ug, uv, cw, cbias, dw):
    ti, tb = position_tables()
    dma = pltpu.SemaphoreType.DMA
    hb = pl.BlockSpec(memory_space=pl.ANY)
    return pl.pallas_call(
        body,
        out_shape=jax.ShapeDtypeStruct((128, 2048), BF16),
        in_specs=[hb] * 16,
        out_specs=hb,
        scratch_shapes=[
            pltpu.VMEM((1024, 256), BF16),
            pltpu.VMEM((1024, 256), BF16),
            pltpu.VMEM((1024, 512), BF16),
            pltpu.VMEM((1024, 512), BF16),
            pltpu.VMEM((8, 128), F32),
            pltpu.VMEM((128, 2048), BF16),
            pltpu.VMEM((512, 2048), BF16),
            pltpu.VMEM((2, 2048), F32),
            pltpu.VMEM((2, 2048), F32),
            pltpu.VMEM((1408, 128), BF16),
            pltpu.VMEM((3, 2, FF), F32),
            pltpu.VMEM((2, FF), F32),
            pltpu.VMEM((2, BLK, 128), F32),
            pltpu.VMEM((8, 128), F32),
            pltpu.VMEM((NSP, 128, 1408), BF16),
            pltpu.VMEM((FFP, 2048), BF16),
            pltpu.VMEM((8, 256), F32),
            pltpu.VMEM((8, 256), F32),
            pltpu.VMEM((256, 8), F32),
            pltpu.VMEM((4, 8, 128), F32),
            pltpu.VMEM((4, 256, 256), BF16),
            pltpu.VMEM((4, 256, 256), BF16),
            pltpu.VMEM((5, 256, 512), F32),
            pltpu.VMEM((4, 256, 512), F32),
            pltpu.VMEM((2, 128, 512), BF16),
            pltpu.VMEM((NSP, 16, 640), BF16),
            pltpu.VMEM((NSP, 16, 640), BF16),
            pltpu.VMEM((NSP, 16, 512), BF16),
            pltpu.VMEM((NSP, 16, 512), BF16),
            pltpu.VMEM((2, 4, 2, 128, 2048), BF16),
            pltpu.VMEM((2, 4, 128, 2048), BF16),
            pltpu.VMEM((2, 3, 128, 2048), BF16),
            pltpu.VMEM((2, 128, 1024), BF16),
            pltpu.VMEM((2, 128, 1024), BF16),
            pltpu.VMEM((2, 128, 2048), BF16),
            pltpu.VMEM((2, 128, 2048), BF16),
            pltpu.VMEM((8, 128, 2048), BF16),
            pltpu.VMEM((1040, 1408), BF16),
            pltpu.VMEM((4, 128, FFP), BF16),
            pltpu.VMEM((4, 128, FFP), BF16),
            pltpu.VMEM((16, 1408), BF16),
            pltpu.VMEM((128, 2048), BF16),
            dma((18,)),
            dma((2,)),
            dma((2,)),
            dma((2,)),
            dma((2, 7)),
            dma((2, 2)),
            dma((2, 2, 4)),
            dma((2, 2)),
            dma((2, 2, 3)),
            dma((2,)),
            dma((2, 9)),
            dma((1,)),
            dma((1,)),
            dma((4,)),
        ],
        compiler_params=pltpu.CompilerParams(
            collective_id=0, has_side_effects=True, vmem_limit_bytes=62 * 1024 * 1024
        ),
        name="layer",
    )(
        q, k, v, g, logd.reshape(8, 128), res, ow, gain, bias, ug.T, uv.T,
        cw.transpose(1, 0, 2), cbias, dw, ti, tb,
    )


def solution(mesh):
    torus = Mesh(mesh.devices.reshape(4, 4, 4, 2), ("z", "y", "x", "c"))
    sp, tp = ("z", "y"), ("x", "c")
    return jax.shard_map(
        shards,
        mesh=torus,
        in_specs=(
            P(sp, tp),
            P(sp, tp),
            P(sp, tp),
            P(sp, tp),
            P(sp, tp),
            P(sp, None),
            P(tp, None),
            P(),
            P(),
            P(sp, tp),
            P(sp, tp),
            P(None, None, tp),
            P(None, tp),
            P(tp, sp),
        ),
        out_specs=P(sp + tp, None),
        check_vma=False,
    )
```
